512 devices in a mesh: sp: 16 (over z), dp: 32 (over y, x, core).
Axes of the slice: x: 4, y: 4, z: 16, core: 2. Of those that a mesh axis runs over, the one named last changes fastest.
Arguments:
- inputs: bfloat16 [32, 2176, 2048], P('dp', 'sp'), may hold values from -6 to 6
- query_vectors: bfloat16 [32, 2176, 1024], P('dp', 'sp'), may hold values from -6 to 6
- key_vectors: bfloat16 [32, 2176, 1024], P('dp', 'sp'), may hold values from -6 to 6
- value_vectors: bfloat16 [32, 2176, 1024], P('dp', 'sp'), may hold values from -6 to 6
- cotangent: bfloat16 [32, 2176, 1024], P('dp', 'sp'), may hold values from -6 to 6
- gate_prefix: float32 [32, 16, 2176], P('dp', 'sp'), may hold values from -2176 to 0, as said below
- value_weight: bfloat16 [2048, 1024], P('sp', 'dp'), may hold values from -0.125 to 0.125
Outputs:
- query_grad: bfloat16 [32, 2176, 1024], P('dp', 'sp')
- key_grad: bfloat16 [32, 2176, 1024], P('dp', 'sp')
- input_grad: bfloat16 [32, 2176, 2048], P('dp', 'sp')
- weight_grad: float32 [2048, 1024], P('sp', 'dp')
The draws below stay inside these ranges and needn't reach their ends.
Inputs may be any that keep to these rules, and one draw needn't show every extreme that they name: `gate_prefix`: non-increasing along the positions of each sequence and head.
All inputs are finite; a program needn't handle non-finite values.
Results may differ from the reference program's by a relative error of at most 0.015.
Values may be sent and summed in bfloat16 or wider, within the bound.
No kernel may reach another device: no remote copies, remote signals or barrier semaphores. Data moves between devices by JAX's collectives and lax.ppermute only.
A program may use at most 128 MiB of HBM per device.

```python
import jax
import jax.numpy as jnp
from jax import lax

MODEL = 2048
HEADS = 16
HEAD_DIM = 64
TOK_DEV = 136
VALUE_WIDTH = 1024
SEQS = 32
LEN = 2176
QBLOCK = 544


def paired_vectors(key):
    folded = jax.random.fold_in(key, 11)
    query_seed, key_seed, spot_seed, sign_seed = jax.random.split(folded, 4)
    shape = (SEQS, LEN, HEADS * HEAD_DIM)
    query_draw = jnp.clip(jax.random.normal(query_seed, shape, jnp.float32), -4.0, 4.0)
    key_draw = jnp.clip(jax.random.normal(key_seed, shape, jnp.float32), -4.0, 4.0)
    return (query_draw, key_draw)


def draw_query_vectors(key, part):
    return paired_vectors(key)[0].astype(jnp.bfloat16)


def draw_key_vectors(key, part):
    return paired_vectors(key)[1].astype(jnp.bfloat16)


def draw_gate_prefix(key, part):
    folded = jax.random.fold_in(key, 23)
    order_seed, fast_seed, slow_seed, step_seed, span_seed = jax.random.split(folded, 5)
    head_order = jax.random.permutation(order_seed, HEADS)
    fast_count = HEADS // 2
    fast_heads = (head_order < fast_count)[None, :, None]
    fast_rate = jax.random.uniform(fast_seed, (SEQS, HEADS, 1), jnp.float32, 0.05, 0.15)
    slow_rate = jax.random.uniform(slow_seed, (SEQS, HEADS, 1), jnp.float32, 0.25, 0.75) / LEN
    step_rate = jnp.where(fast_heads, fast_rate, slow_rate)
    step_factor = jax.random.uniform(step_seed, (SEQS, HEADS, LEN), jnp.float32, 0.5, 1.5)
    span_factor = jnp.exp(jax.random.uniform(span_seed, (SEQS, HEADS, LEN // TOK_DEV), jnp.float32, -0.6931, 0.6931))
    span_factor = jnp.repeat(span_factor, TOK_DEV, axis=2)
    log_steps = -step_rate * step_factor * span_factor
    return jnp.cumsum(log_steps, axis=2)


def steps_of(key, extent, shards, low, largest):
    loudness = 1.0
    for position, shards_of in shards:
        heights = jax.random.uniform(jax.random.fold_in(jax.random.fold_in(key, 6), position), (shards_of,), jnp.float32, low / len(shards), largest / len(shards))
        loudness = loudness * jnp.repeat(jnp.exp(heights), extent[position] // shards_of).reshape((-1,) + (1,) * (len(extent) - 1 - position))
    return loudness


def noise(rng, dims, spread, limit, shards=(), kind=jnp.bfloat16):
    drawn = jax.random.normal(rng, dims, jnp.float32) * spread
    if len(shards) > 0:
        drawn = steps_of(rng, dims, shards, -0.22, 0.18) * drawn
    return jnp.clip(drawn, min=-limit, max=limit).astype(kind)


def setup_inputs(seed: int = 0) -> dict:
    key_of = jax.random.split(jax.random.key(seed), 8)
    return {
        "inputs": noise(key_of[0], (SEQS, LEN, MODEL), 1.0, 6.0, ((0, 32), (1, 16))),
        "query_vectors": draw_query_vectors(jax.random.fold_in(key_of[7], 71), 0),
        "key_vectors": draw_key_vectors(jax.random.fold_in(key_of[7], 71), 0),
        "value_vectors": noise(key_of[3], (SEQS, LEN, VALUE_WIDTH), 1.0, 6.0, ((0, 32), (1, 16))),
        "cotangent": noise(key_of[4], (SEQS, LEN, VALUE_WIDTH), 1.0, 6.0, ((0, 32), (1, 16))),
        "gate_prefix": draw_gate_prefix(jax.random.fold_in(key_of[7], 71), 0),
        "value_weight": noise(key_of[6], (MODEL, VALUE_WIDTH), MODEL ** -0.5, 0.125, ((0, 16), (1, 32))),
    }


def sequence_backward(query_heads, key_heads, value_heads, grad_heads, prefix):
    score_scale = HEAD_DIM ** -0.5
    query_wide = query_heads.astype(jnp.float32)
    key_wide = key_heads.astype(jnp.float32)
    value_wide = value_heads.astype(jnp.float32)
    grad_wide = grad_heads.astype(jnp.float32)
    key_accum = jnp.zeros(key_wide.shape, jnp.float32)
    value_accum = jnp.zeros(key_wide.shape, jnp.float32)
    query_parts = []
    for block_index in range(LEN // QBLOCK):
        first_row = block_index * QBLOCK
        last_row = first_row + QBLOCK
        query_rows = query_wide[first_row:last_row]
        key_rows = key_wide[:last_row]
        grad_rows = grad_wide[first_row:last_row]
        scores = jnp.einsum('qhd,khd->hqk', query_rows, key_rows) * score_scale
        scores = scores + prefix[:, first_row:last_row, None] - prefix[:, None, :last_row]
        causal = jnp.arange(last_row)[None, :] <= (first_row + jnp.arange(QBLOCK))[:, None]
        scores = jnp.where(causal[None], scores, -jnp.inf)
        row_peak = jnp.max(scores, axis=-1, keepdims=True)
        raised_scores = jnp.exp(scores - row_peak)
        softmax_rows = raised_scores / jnp.sum(raised_scores, axis=-1, keepdims=True)
        softmax_low = lax.optimization_barrier(softmax_rows.astype(jnp.bfloat16)).astype(jnp.float32)
        value_accum = value_accum.at[:last_row].add(jnp.einsum('hqk,qhd->khd', softmax_low, grad_rows))
        softmax_grad = jnp.einsum('qhd,khd->hqk', grad_rows, value_wide[:last_row])
        row_term = jnp.sum(softmax_rows * softmax_grad, axis=-1, keepdims=True)
        score_grad = softmax_rows * (softmax_grad - row_term)
        score_low = lax.optimization_barrier(score_grad.astype(jnp.bfloat16)).astype(jnp.float32)
        query_parts.append((jnp.einsum('hqk,khd->qhd', score_low, key_rows) * score_scale).astype(jnp.bfloat16))
        key_accum = key_accum.at[:last_row].add(jnp.einsum('hqk,qhd->khd', score_low, query_rows))
    query_grad = jnp.concatenate(query_parts, axis=0)
    key_grad = (key_accum * score_scale).astype(jnp.bfloat16)
    return query_grad, key_grad, value_accum.astype(jnp.bfloat16)


def reference(inputs, query_vectors, key_vectors, value_vectors, cotangent, gate_prefix, value_weight):
    head_shape = (LEN, HEADS, HEAD_DIM)

    def per_sequence(weight_total, sequence_items):
        seq_inputs, seq_query, seq_key, seq_value, seq_grad, seq_prefix = sequence_items
        query_grad, key_grad, value_grad = sequence_backward(
            seq_query.reshape(head_shape), seq_key.reshape(head_shape),
            seq_value.reshape(head_shape), seq_grad.reshape(head_shape), seq_prefix)
        value_flat = value_grad.reshape(LEN, VALUE_WIDTH)
        input_grad = jnp.dot(value_flat, value_weight.T, preferred_element_type=jnp.float32).astype(jnp.bfloat16)
        weight_total = weight_total + jnp.dot(seq_inputs.T, value_flat, preferred_element_type=jnp.float32)
        return weight_total, (query_grad.reshape(LEN, VALUE_WIDTH), key_grad.reshape(LEN, VALUE_WIDTH), input_grad)

    weight_total, outputs = lax.scan(
        per_sequence, jnp.zeros((MODEL, VALUE_WIDTH), jnp.float32),
        (inputs, query_vectors, key_vectors, value_vectors, cotangent, gate_prefix))
    query_grad, key_grad, input_grad = outputs
    return (query_grad, key_grad, input_grad, weight_total)
```

```python
import jax
import jax.numpy as jnp
from jax import lax
from jax.experimental import pallas as pl
from jax.experimental.pallas import tpu as pltpu
from jax.sharding import Mesh, PartitionSpec as P

HEAD_DIM = 64
LANES = 128
TILE = 256
FLOOR = -1e30


def rolled(x):
    return pltpu.roll(x, HEAD_DIM, 1)


def low_lanes(shape):
    return lax.broadcasted_iota(jnp.int32, shape, 1) < HEAD_DIM


def pack_kernel(q_ref, k_ref, v_ref, g_ref, w_ref, out_ref):
    heads, rows, _ = out_ref.shape
    tokens = q_ref.shape[0]
    low = low_lanes((tokens, LANES))
    half = w_ref.shape[0] // 2
    for pair in range(heads // 2):
        cols = slice(pair * LANES, (pair + 1) * LANES)
        for first_ref, second_ref, lane in ((q_ref, k_ref, 0), (v_ref, g_ref, LANES)):
            first = first_ref[:, cols].astype(jnp.float32)
            second = second_ref[:, cols].astype(jnp.float32)
            out_ref[2 * pair, :tokens, lane : lane + LANES] = jnp.where(
                low, first, rolled(second)
            ).astype(jnp.bfloat16)
            out_ref[2 * pair + 1, :tokens, lane : lane + LANES] = jnp.where(
                low, rolled(first), second
            ).astype(jnp.bfloat16)
    for head in range(heads):
        out_ref[head, tokens:rows, :LANES] = w_ref[:half]
        out_ref[head, tokens:rows, LANES:] = w_ref[half:]


def unpack_weight_kernel(x_ref, out_ref):
    planes, half, _ = x_ref.shape
    for plane in range(planes):
        cols = slice(plane * LANES, (plane + 1) * LANES)
        out_ref[:half, cols] = x_ref[plane, :, :LANES]
        out_ref[half:, cols] = x_ref[plane, :, LANES:]


def dot_nt(a, b):
    return lax.dot_general(a, b, (((1,), (1,)), ((), ())), preferred_element_type=jnp.float32)


def dot_nn(a, b):
    return lax.dot_general(a, b, (((1,), (0,)), ((), ())), preferred_element_type=jnp.float32)


def folded(x, op):
    return op(x.reshape(x.shape[0] // 8, 8, x.shape[1]), axis=0)


def attention_kernel(
    x_ref, p_ref, qk_ref, v_out_ref, kq_ref, kt_ref, pc_ref, acc_ref, dq_ref, s_ref, d_ref
):
    length = x_ref.shape[0]
    scale = HEAD_DIM**-0.5
    blocks = [(b, min(TILE, length - b)) for b in range(0, length, TILE)]
    for base, rows in blocks:
        here = slice(base, base + rows)
        wide = x_ref[here, :LANES].astype(jnp.float32)
        swapped = rolled(wide)
        kq_ref[here] = swapped.astype(jnp.bfloat16)
        kt_ref[:, here] = swapped.T[:HEAD_DIM].astype(jnp.bfloat16)
        pc_ref[here] = jnp.broadcast_to(p_ref[:, here], (LANES, rows)).T
        acc_ref[here] = jnp.zeros((rows, LANES), jnp.float32)
    for index, (q_base, q_rows) in enumerate(blocks):
        q_here = slice(q_base, q_base + q_rows)
        low = low_lanes((q_rows, LANES))
        query_wide = x_ref[q_here, :LANES].astype(jnp.float32)
        grad_wide = rolled(x_ref[q_here, LANES:].astype(jnp.float32))
        query_low = jnp.where(low, query_wide * scale, 0.0).astype(jnp.bfloat16)
        query_high = jnp.where(low, 0.0, rolled(query_wide)).astype(jnp.bfloat16)
        grad_low = jnp.where(low, grad_wide, 0.0).astype(jnp.bfloat16)
        pivot = pc_ref[q_base : q_base + 1, :]
        peak = jnp.full((8, q_rows), FLOOR, jnp.float32)
        for u_base, u_rows in blocks[: index + 1]:
            u_here = slice(u_base, u_base + u_rows)
            shift = pivot - pc_ref[u_here]
            shift = jnp.concatenate([shift] * (q_rows // LANES), axis=1)
            scores = dot_nt(kq_ref[u_here], query_low) + shift
            if u_base == q_base:
                seen = lax.broadcasted_iota(jnp.int32, scores.shape, 0) <= lax.broadcasted_iota(
                    jnp.int32, scores.shape, 1
                )
                scores = jnp.where(seen, scores, FLOOR)
            s_ref[u_here, :q_rows] = scores
            peak = jnp.maximum(peak, folded(scores, jnp.max))
        peak = jnp.max(peak, axis=0, keepdims=True)
        total = jnp.zeros((8, q_rows), jnp.float32)
        for u_base, u_rows in blocks[: index + 1]:
            u_here = slice(u_base, u_base + u_rows)
            raised = jnp.exp(s_ref[u_here, :q_rows] - peak)
            s_ref[u_here, :q_rows] = raised
            total = total + folded(raised, jnp.sum)
        share = 1.0 / jnp.sum(total, axis=0, keepdims=True)
        term = jnp.zeros((8, q_rows), jnp.float32)
        for u_base, u_rows in blocks[: index + 1]:
            u_here = slice(u_base, u_base + u_rows)
            soft = s_ref[u_here, :q_rows] * share
            s_ref[u_here, :q_rows] = soft
            acc_ref[u_here] += dot_nn(soft.astype(jnp.bfloat16), grad_low)
            soft_grad = dot_nt(x_ref[u_here, LANES:], grad_low)
            d_ref[u_here, :q_rows] = soft_grad
            term = term + folded(soft * soft_grad, jnp.sum)
        term = jnp.sum(term, axis=0, keepdims=True)
        query_grad = jnp.zeros((HEAD_DIM, q_rows), jnp.float32)
        for u_base, u_rows in blocks[: index + 1]:
            u_here = slice(u_base, u_base + u_rows)
            score_low = (s_ref[u_here, :q_rows] * (d_ref[u_here, :q_rows] - term)).astype(
                jnp.bfloat16
            )
            acc_ref[u_here] += dot_nn(score_low, query_high)
            query_grad = query_grad + dot_nn(kt_ref[:, u_here], score_low)
        query_grad = jnp.concatenate([query_grad, jnp.zeros_like(query_grad)], axis=0)
        dq_ref[q_here] = query_grad.T
    for base, rows in blocks:
        here = slice(base, base + rows)
        qk_ref[here] = (
            jnp.where(low_lanes((rows, LANES)), dq_ref[here], acc_ref[here]) * scale
        ).astype(jnp.bfloat16)
    planes, kept, _ = v_out_ref.shape
    tokens = length // planes
    for plane in range(planes):
        base = plane * tokens
        first = acc_ref[base : base + kept]
        second = acc_ref[base + kept : base + tokens]
        second = jnp.concatenate([second, first[: 2 * kept - tokens]], axis=0)
        v_out_ref[plane] = jnp.where(low_lanes(first.shape), first, rolled(second)).astype(
            jnp.bfloat16
        )


def unpack_value_kernel(x_ref, out_ref):
    heads, kept, _ = x_ref.shape
    rest = out_ref.shape[0] - kept
    low = low_lanes((kept, LANES))
    for pair in range(heads // 2):
        first = x_ref[2 * pair].astype(jnp.float32)
        second = x_ref[2 * pair + 1].astype(jnp.float32)
        top = jnp.where(low, first, rolled(second))
        bottom = jnp.where(low, rolled(first), second)[:rest]
        out_ref[:, pair * LANES : (pair + 1) * LANES] = jnp.concatenate(
            [top, bottom], axis=0
        ).astype(jnp.bfloat16)


def unpack_pair_kernel(x_ref, q_ref, k_ref):
    heads, tokens, _ = x_ref.shape
    low = low_lanes((tokens, LANES))
    for pair in range(heads // 2):
        first = x_ref[2 * pair].astype(jnp.float32)
        second = x_ref[2 * pair + 1].astype(jnp.float32)
        cols = slice(pair * LANES, (pair + 1) * LANES)
        q_ref[:, cols] = jnp.where(low, first, rolled(second)).astype(jnp.bfloat16)
        k_ref[:, cols] = jnp.where(low, rolled(first), second).astype(jnp.bfloat16)


def exchanged(x, axis):
    return lax.all_to_all(x, axis, split_axis=0, concat_axis=0, tiled=True)


def shaped(*shape, dtype=jnp.bfloat16):
    return jax.ShapeDtypeStruct(shape, dtype)


def shards(inputs, query_vectors, key_vectors, value_vectors, cotangent, gate_prefix, value_weight):
    planes = lax.axis_size("sp")
    tokens, model = inputs.shape[1:]
    width = query_vectors.shape[2]
    heads = width // HEAD_DIM
    length = planes * tokens
    w_cols = value_weight.shape[1]
    packed = pl.pallas_call(
        pack_kernel, out_shape=shaped(heads, tokens + w_cols // 2, 2 * LANES)
    )(query_vectors[0], key_vectors[0], value_vectors[0], cotangent[0], value_weight.T)
    arrived = exchanged(packed, "sp")
    weight_block = pl.pallas_call(unpack_weight_kernel, out_shape=shaped(w_cols, model))(
        arrived[:, tokens:]
    )
    weight_all = lax.all_gather(weight_block, "dp", axis=0, tiled=True)
    kept = (tokens // 2 + 7) // 8 * 8
    pair_grad, value_grad = pl.pallas_call(
        attention_kernel,
        out_shape=(shaped(length, LANES), shaped(planes, kept, LANES)),
        scratch_shapes=[
            pltpu.VMEM((length, LANES), jnp.bfloat16),
            pltpu.VMEM((HEAD_DIM, length), jnp.bfloat16),
            pltpu.VMEM((length, LANES), jnp.float32),
            pltpu.VMEM((length, LANES), jnp.float32),
            pltpu.VMEM((length, LANES), jnp.float32),
            pltpu.VMEM((length, TILE), jnp.float32),
            pltpu.VMEM((length, TILE), jnp.float32),
        ],
    )(arrived[:, :tokens].reshape(length, 2 * LANES), gate_prefix[0])
    value_back = exchanged(value_grad, "sp")
    value_rows = pl.pallas_call(unpack_value_kernel, out_shape=shaped(tokens, width))(value_back)
    partial = lax.dot_general(
        value_rows, inputs[0], (((0,), (0,)), ((), ())), preferred_element_type=jnp.float32
    ).astype(jnp.bfloat16)
    partial = exchanged(partial, "dp").reshape(lax.axis_size("dp"), w_cols, model)
    partial = partial.astype(jnp.float32).sum(axis=0).astype(jnp.bfloat16)
    partial = jnp.moveaxis(partial.reshape(w_cols, planes, model // planes), 1, 0)
    weight_grad = exchanged(partial, "sp").astype(jnp.float32).sum(axis=0).T
    pair_back = exchanged(pair_grad.reshape(planes, tokens, LANES), "sp")
    query_grad, key_grad = pl.pallas_call(
        unpack_pair_kernel, out_shape=(shaped(tokens, width), shaped(tokens, width))
    )(pair_back)
    input_grad = lax.dot_general(
        value_rows, weight_all, (((1,), (0,)), ((), ())), preferred_element_type=jnp.float32
    ).astype(jnp.bfloat16)
    return (query_grad[None], key_grad[None], input_grad[None], weight_grad)


def solution(mesh):
    in_specs = (P("dp", "sp", None),) * 6 + (P("sp", "dp"),)
    out_specs = (P("dp", "sp", None), P("dp", "sp", None), P("dp", "sp", None), P("sp", "dp"))
    return jax.shard_map(shards, mesh=mesh, in_specs=in_specs, out_specs=out_specs, check_vma=False)
```

```python
import jax
import jax.numpy as jnp
from jax import lax
from jax.experimental import pallas as pl
from jax.experimental.pallas import tpu as pltpu
from jax.sharding import Mesh, PartitionSpec as P

HEAD_DIM = 64
LANES = 128
TILE = 256
FLOOR = -1e30


def rolled(x):
    return pltpu.roll(x, HEAD_DIM, 1)


def low_lanes(shape):
    return lax.broadcasted_iota(jnp.int32, shape, 1) < HEAD_DIM


def pack_kernel(q_ref, k_ref, v_ref, g_ref, w_ref, out_ref):
    heads, rows, _ = out_ref.shape
    tokens = q_ref.shape[0]
    low = low_lanes((tokens, LANES))
    half = w_ref.shape[0] // 2
    for pair in range(heads // 2):
        cols = slice(pair * LANES, (pair + 1) * LANES)
        for first_ref, second_ref, lane in ((q_ref, k_ref, 0), (v_ref, g_ref, LANES)):
            first = first_ref[:, cols].astype(jnp.float32)
            second = second_ref[:, cols].astype(jnp.float32)
            out_ref[2 * pair, :tokens, lane : lane + LANES] = jnp.where(
                low, first, rolled(second)
            ).astype(jnp.bfloat16)
            out_ref[2 * pair + 1, :tokens, lane : lane + LANES] = jnp.where(
                low, rolled(first), second
            ).astype(jnp.bfloat16)
    for head in range(heads):
        out_ref[head, tokens:rows, :LANES] = w_ref[:half]
        out_ref[head, tokens:rows, LANES:] = w_ref[half:]


def unpack_weight_kernel(x_ref, out_ref):
    planes, half, _ = x_ref.shape
    for plane in range(planes):
        cols = slice(plane * LANES, (plane + 1) * LANES)
        out_ref[:half, cols] = x_ref[plane, :, :LANES]
        out_ref[half:, cols] = x_ref[plane, :, LANES:]


def dot_nt(a, b):
    return lax.dot_general(a, b, (((1,), (1,)), ((), ())), preferred_element_type=jnp.float32)


def dot_nn(a, b):
    return lax.dot_general(a, b, (((1,), (0,)), ((), ())), preferred_element_type=jnp.float32)


def folded(x, op):
    return op(x.reshape(x.shape[0] // 8, 8, x.shape[1]), axis=0)


def attention_kernel(
    x_ref, p_ref, qk_ref, v_out_ref, kq_ref, kt_ref, pc_ref, acc_ref, dq_ref, s_ref, d_ref
):
    length = x_ref.shape[0]
    scale = HEAD_DIM**-0.5
    blocks = [(b, min(TILE, length - b)) for b in range(0, length, TILE)]
    for base, rows in blocks:
        here = slice(base, base + rows)
        wide = x_ref[here, :LANES].astype(jnp.float32)
        swapped = rolled(wide)
        kq_ref[here] = swapped.astype(jnp.bfloat16)
        kt_ref[:, here] = swapped.T[:HEAD_DIM].astype(jnp.bfloat16)
        pc_ref[here] = jnp.broadcast_to(p_ref[:, here], (LANES, rows)).T
        acc_ref[here] = jnp.zeros((rows, LANES), jnp.float32)
    for index, (q_base, q_rows) in enumerate(blocks):
        q_here = slice(q_base, q_base + q_rows)
        low = low_lanes((q_rows, LANES))
        query_wide = x_ref[q_here, :LANES].astype(jnp.float32)
        grad_wide = rolled(x_ref[q_here, LANES:].astype(jnp.float32))
        query_low = jnp.where(low, query_wide * scale, 0.0).astype(jnp.bfloat16)
        query_high = jnp.where(low, 0.0, rolled(query_wide)).astype(jnp.bfloat16)
        grad_low = jnp.where(low, grad_wide, 0.0).astype(jnp.bfloat16)
        pivot = pc_ref[q_base : q_base + 1, :]
        peak = jnp.full((8, q_rows), FLOOR, jnp.float32)
        for u_base, u_rows in blocks[: index + 1]:
            u_here = slice(u_base, u_base + u_rows)
            shift = pivot - pc_ref[u_here]
            shift = jnp.concatenate([shift] * (q_rows // LANES), axis=1)
            scores = dot_nt(kq_ref[u_here], query_low) + shift
            if u_base == q_base:
                seen = lax.broadcasted_iota(jnp.int32, scores.shape, 0) <= lax.broadcasted_iota(
                    jnp.int32, scores.shape, 1
                )
                scores = jnp.where(seen, scores, FLOOR)
            s_ref[u_here, :q_rows] = scores
            peak = jnp.maximum(peak, folded(scores, jnp.max))
        peak = jnp.max(peak, axis=0, keepdims=True)
        total = jnp.zeros((8, q_rows), jnp.float32)
        for u_base, u_rows in blocks[: index + 1]:
            u_here = slice(u_base, u_base + u_rows)
            raised = jnp.exp(s_ref[u_here, :q_rows] - peak)
            s_ref[u_here, :q_rows] = raised
            total = total + folded(raised, jnp.sum)
        share = 1.0 / jnp.sum(total, axis=0, keepdims=True)
        term = jnp.zeros((8, q_rows), jnp.float32)
        for u_base, u_rows in blocks[: index + 1]:
            u_here = slice(u_base, u_base + u_rows)
            soft = s_ref[u_here, :q_rows] * share
            s_ref[u_here, :q_rows] = soft
            acc_ref[u_here] += dot_nn(soft.astype(jnp.bfloat16), grad_low)
            soft_grad = dot_nt(x_ref[u_here, LANES:], grad_low)
            d_ref[u_here, :q_rows] = soft_grad
            term = term + folded(soft * soft_grad, jnp.sum)
        term = jnp.sum(term, axis=0, keepdims=True)
        query_grad = jnp.zeros((HEAD_DIM, q_rows), jnp.float32)
        for u_base, u_rows in blocks[: index + 1]:
            u_here = slice(u_base, u_base + u_rows)
            score_low = (s_ref[u_here, :q_rows] * (d_ref[u_here, :q_rows] - term)).astype(
                jnp.bfloat16
            )
            acc_ref[u_here] += dot_nn(score_low, query_high)
            query_grad = query_grad + dot_nn(kt_ref[:, u_here], score_low)
        query_grad = jnp.concatenate([query_grad, jnp.zeros_like(query_grad)], axis=0)
        dq_ref[q_here] = query_grad.T
    for base, rows in blocks:
        here = slice(base, base + rows)
        qk_ref[here] = (
            jnp.where(low_lanes((rows, LANES)), dq_ref[here], acc_ref[here]) * scale
        ).astype(jnp.bfloat16)
    planes, kept, _ = v_out_ref.shape
    tokens = length // planes
    for plane in range(planes):
        base = plane * tokens
        first = acc_ref[base : base + kept]
        second = acc_ref[base + kept : base + tokens]
        second = jnp.concatenate([second, first[: 2 * kept - tokens]], axis=0)
        v_out_ref[plane] = jnp.where(low_lanes(first.shape), first, rolled(second)).astype(
            jnp.bfloat16
        )


def unpack_value_kernel(x_ref, rows_ref, parts_ref):
    heads, kept, _ = x_ref.shape
    cores, columns, tokens, _ = parts_ref.shape
    rest = tokens - kept
    quarter = LANES // heads * columns
    lane = lax.broadcasted_iota(jnp.int32, (tokens, LANES), 1)
    for column in range(columns):
        parts = [jnp.zeros((tokens, LANES), jnp.float32)] * cores
        for group in range(heads // columns):
            block = x_ref[group * columns + column].astype(jnp.float32)
            for core in range(cores):
                home = group * quarter
                top = pltpu.roll(block, (home - core * quarter) % LANES, 1)
                bottom = pltpu.roll(block, (home - core * quarter - HEAD_DIM) % LANES, 1)[:rest]
                moved = jnp.concatenate([top, bottom], axis=0)
                inside = (lane >= home) & (lane < home + quarter)
                parts[core] = jnp.where(inside, moved, parts[core])
        for core in range(cores):
            part = parts[core].astype(jnp.bfloat16)
            parts_ref[core, column] = part
            rows_ref[core, :, column * LANES : (column + 1) * LANES] = part


def unpack_pair_kernel(x_ref, q_ref, k_ref):
    heads, tokens, _ = x_ref.shape
    low = low_lanes((tokens, LANES))
    for pair in range(heads // 2):
        first = x_ref[2 * pair].astype(jnp.float32)
        second = x_ref[2 * pair + 1].astype(jnp.float32)
        cols = slice(pair * LANES, (pair + 1) * LANES)
        q_ref[:, cols] = jnp.where(low, first, rolled(second)).astype(jnp.bfloat16)
        k_ref[:, cols] = jnp.where(low, rolled(first), second).astype(jnp.bfloat16)


def exchanged(x, axis):
    return lax.all_to_all(x, axis, split_axis=0, concat_axis=0, tiled=True)


def shifted(x, axis, step):
    count = lax.axis_size(axis)
    return lax.ppermute(x, axis, [(place, (place + step) % count) for place in range(count)])


def block_of(x, index):
    return lax.dynamic_index_in_dim(x, index, 0, keepdims=False)


def from_all(x, axis):
    return [x] + [shifted(x, axis, step) for step in range(1, lax.axis_size(axis))]


def sent_blocks(blocks, axis):
    count = lax.axis_size(axis)
    here = lax.axis_index(axis)
    own = block_of(blocks, here)
    return [own] + [
        shifted(block_of(blocks, (here + step) % count), axis, step) for step in range(1, count)
    ]


def placed(parts, axis):
    count = lax.axis_size(axis)
    here = lax.axis_index(axis)
    whole = jnp.zeros((count, *parts[0].shape), parts[0].dtype)
    for step, part in enumerate(parts):
        whole = lax.dynamic_update_index_in_dim(whole, part, (here - step) % count, 0)
    return whole.reshape(count * parts[0].shape[0], *parts[0].shape[1:])


def shaped(*shape, dtype=jnp.bfloat16):
    return jax.ShapeDtypeStruct(shape, dtype)


def shards(inputs, query_vectors, key_vectors, value_vectors, cotangent, gate_prefix, value_weight):
    planes = lax.axis_size("sp")
    cores, columns, lines = lax.axis_size("core"), lax.axis_size("x"), lax.axis_size("y")
    core = lax.axis_index("core")
    tokens, model = inputs.shape[1:]
    width = query_vectors.shape[2]
    heads = width // HEAD_DIM
    length = planes * tokens
    w_cols = value_weight.shape[1]
    packed = pl.pallas_call(
        pack_kernel, out_shape=shaped(heads, tokens + w_cols // 2, 2 * LANES)
    )(query_vectors[0], key_vectors[0], value_vectors[0], cotangent[0], value_weight.T)
    arrived = exchanged(packed, "sp")
    input_rows = jnp.concatenate(from_all(inputs[0], "x"), axis=0)
    input_rows = jnp.concatenate(from_all(input_rows, "core"), axis=0)
    weight_block = pl.pallas_call(unpack_weight_kernel, out_shape=shaped(w_cols, model))(
        arrived[:, tokens:]
    )
    weight_line = placed(from_all(weight_block, "y"), "y")
    weight_half = placed(from_all(weight_line, "x"), "x")
    weight_halves = from_all(weight_half, "core")
    kept = (tokens // 2 + 7) // 8 * 8
    pair_grad, value_grad = pl.pallas_call(
        attention_kernel,
        out_shape=(shaped(length, LANES), shaped(planes, kept, LANES)),
        scratch_shapes=[
            pltpu.VMEM((length, LANES), jnp.bfloat16),
            pltpu.VMEM((HEAD_DIM, length), jnp.bfloat16),
            pltpu.VMEM((length, LANES), jnp.float32),
            pltpu.VMEM((length, LANES), jnp.float32),
            pltpu.VMEM((length, LANES), jnp.float32),
            pltpu.VMEM((length, TILE), jnp.float32),
            pltpu.VMEM((length, TILE), jnp.float32),
        ],
    )(arrived[:, :tokens].reshape(length, 2 * LANES), gate_prefix[0])
    value_back = exchanged(value_grad, "sp")
    value_rows, value_parts = pl.pallas_call(
        unpack_value_kernel,
        out_shape=(
            shaped(cores, tokens, width // cores),
            shaped(cores, columns, tokens, LANES),
        ),
    )(value_back)
    pair_back = exchanged(pair_grad.reshape(planes, tokens, LANES), "sp")
    both = jnp.concatenate(
        [block_of(value_parts, core), shifted(block_of(value_parts, 1 - core), "core", 1)], axis=1
    )
    pieces = sent_blocks(both, "x")
    value_cols = jnp.concatenate(
        [piece[:tokens] for piece in pieces] + [piece[tokens:] for piece in pieces], axis=0
    )
    partial = lax.dot_general(
        value_cols, input_rows, (((0,), (0,)), ((), ())), preferred_element_type=jnp.float32
    ).astype(jnp.bfloat16)
    partial = sent_blocks(partial.reshape(lines, w_cols, model), "y")
    partial = sum(part.astype(jnp.float32) for part in partial).astype(jnp.bfloat16)
    partial = jnp.moveaxis(partial.reshape(w_cols, planes, model // planes), 1, 0)
    weight_grad = exchanged(partial, "sp").astype(jnp.float32).sum(axis=0).T
    query_grad, key_grad = pl.pallas_call(
        unpack_pair_kernel, out_shape=(shaped(tokens, width), shaped(tokens, width))
    )(pair_back)
    input_grad = sum(
        lax.dot_general(
            block_of(value_rows, place),
            half,
            (((1,), (0,)), ((), ())),
            preferred_element_type=jnp.float32,
        )
        for place, half in zip((core, 1 - core), weight_halves)
    ).astype(jnp.bfloat16)
    return (query_grad[None], key_grad[None], input_grad[None], weight_grad)


def solution(mesh):
    grid = Mesh(mesh.devices.reshape(-1, 4, 4, 2), ("sp", "y", "x", "core"))
    rows = P(("y", "x", "core"), "sp", None)
    weight = P("sp", ("y", "x", "core"))
    return jax.shard_map(
        shards,
        mesh=grid,
        in_specs=(rows,) * 6 + (weight,),
        out_specs=(rows, rows, rows, weight),
        check_vma=False,
    )
```

```python
import jax
import jax.numpy as jnp
from jax import lax
from jax.experimental import pallas as pl
from jax.experimental.pallas import tpu as pltpu
from jax.sharding import Mesh, PartitionSpec as P

HEAD_DIM = 64
LANES = 128
TILE = 256
FLOOR = -1e30


def rolled(x):
    return pltpu.roll(x, HEAD_DIM, 1)


def low_lanes(shape):
    return lax.broadcasted_iota(jnp.int32, shape, 1) < HEAD_DIM


def pack_kernel(q_ref, k_ref, v_ref, g_ref, out_ref):
    heads, tokens, _ = out_ref.shape
    low = low_lanes((tokens, LANES))
    for pair in range(heads // 2):
        cols = slice(pair * LANES, (pair + 1) * LANES)
        for first_ref, second_ref, lane in ((q_ref, k_ref, 0), (v_ref, g_ref, LANES)):
            first = first_ref[:, cols].astype(jnp.float32)
            second = second_ref[:, cols].astype(jnp.float32)
            out_ref[2 * pair, :, lane : lane + LANES] = jnp.where(
                low, first, rolled(second)
            ).astype(jnp.bfloat16)
            out_ref[2 * pair + 1, :, lane : lane + LANES] = jnp.where(
                low, rolled(first), second
            ).astype(jnp.bfloat16)


def dot_nt(a, b):
    return lax.dot_general(a, b, (((1,), (1,)), ((), ())), preferred_element_type=jnp.float32)


def dot_nn(a, b):
    return lax.dot_general(a, b, (((1,), (0,)), ((), ())), preferred_element_type=jnp.float32)


def folded(x, op):
    return op(x.reshape(x.shape[0] // 8, 8, x.shape[1]), axis=0)


def attention_kernel(
    x_ref, p_ref, qk_ref, v_out_ref, kq_ref, kt_ref, pc_ref, acc_ref, dq_ref, s_ref, d_ref
):
    length = x_ref.shape[0]
    scale = HEAD_DIM**-0.5
    blocks = [(b, min(TILE, length - b)) for b in range(0, length, TILE)]
    for base, rows in blocks:
        here = slice(base, base + rows)
        wide = x_ref[here, :LANES].astype(jnp.float32)
        swapped = rolled(wide)
        kq_ref[here] = swapped.astype(jnp.bfloat16)
        kt_ref[:, here] = swapped.T[:HEAD_DIM].astype(jnp.bfloat16)
        pc_ref[here] = jnp.broadcast_to(p_ref[:, here], (LANES, rows)).T
        acc_ref[here] = jnp.zeros((rows, LANES), jnp.float32)
    for index, (q_base, q_rows) in enumerate(blocks):
        q_here = slice(q_base, q_base + q_rows)
        low = low_lanes((q_rows, LANES))
        query_wide = x_ref[q_here, :LANES].astype(jnp.float32)
        grad_wide = rolled(x_ref[q_here, LANES:].astype(jnp.float32))
        query_low = jnp.where(low, query_wide * scale, 0.0).astype(jnp.bfloat16)
        query_high = jnp.where(low, 0.0, rolled(query_wide)).astype(jnp.bfloat16)
        grad_low = jnp.where(low, grad_wide, 0.0).astype(jnp.bfloat16)
        pivot = pc_ref[q_base : q_base + 1, :]
        peak = jnp.full((8, q_rows), FLOOR, jnp.float32)
        for u_base, u_rows in blocks[: index + 1]:
            u_here = slice(u_base, u_base + u_rows)
            shift = pivot - pc_ref[u_here]
            shift = jnp.concatenate([shift] * (q_rows // LANES), axis=1)
            scores = dot_nt(kq_ref[u_here], query_low) + shift
            if u_base == q_base:
                seen = lax.broadcasted_iota(jnp.int32, scores.shape, 0) <= lax.broadcasted_iota(
                    jnp.int32, scores.shape, 1
                )
                scores = jnp.where(seen, scores, FLOOR)
            s_ref[u_here, :q_rows] = scores
            peak = jnp.maximum(peak, folded(scores, jnp.max))
        peak = jnp.max(peak, axis=0, keepdims=True)
        total = jnp.zeros((8, q_rows), jnp.float32)
        for u_base, u_rows in blocks[: index + 1]:
            u_here = slice(u_base, u_base + u_rows)
            raised = jnp.exp(s_ref[u_here, :q_rows] - peak)
            s_ref[u_here, :q_rows] = raised
            total = total + folded(raised, jnp.sum)
        share = 1.0 / jnp.sum(total, axis=0, keepdims=True)
        term = jnp.zeros((8, q_rows), jnp.float32)
        for u_base, u_rows in blocks[: index + 1]:
            u_here = slice(u_base, u_base + u_rows)
            soft = s_ref[u_here, :q_rows] * share
            s_ref[u_here, :q_rows] = soft
            acc_ref[u_here] += dot_nn(soft.astype(jnp.bfloat16), grad_low)
            soft_grad = dot_nt(x_ref[u_here, LANES:], grad_low)
            d_ref[u_here, :q_rows] = soft_grad
            term = term + folded(soft * soft_grad, jnp.sum)
        term = jnp.sum(term, axis=0, keepdims=True)
        query_grad = jnp.zeros((HEAD_DIM, q_rows), jnp.float32)
        for u_base, u_rows in blocks[: index + 1]:
            u_here = slice(u_base, u_base + u_rows)
            score_low = (s_ref[u_here, :q_rows] * (d_ref[u_here, :q_rows] - term)).astype(
                jnp.bfloat16
            )
            acc_ref[u_here] += dot_nn(score_low, query_high)
            query_grad = query_grad + dot_nn(kt_ref[:, u_here], score_low)
        query_grad = jnp.concatenate([query_grad, jnp.zeros_like(query_grad)], axis=0)
        dq_ref[q_here] = query_grad.T
    for base, rows in blocks:
        here = slice(base, base + rows)
        qk_ref[here] = (
            jnp.where(low_lanes((rows, LANES)), dq_ref[here], acc_ref[here]) * scale
        ).astype(jnp.bfloat16)
    planes, kept, _ = v_out_ref.shape
    tokens = length // planes
    for plane in range(planes):
        base = plane * tokens
        first = acc_ref[base : base + kept]
        second = acc_ref[base + kept : base + tokens]
        second = jnp.concatenate([second, first[: 2 * kept - tokens]], axis=0)
        v_out_ref[plane] = jnp.where(low_lanes(first.shape), first, rolled(second)).astype(
            jnp.bfloat16
        )


def unpack_value_kernel(x_ref, rows_ref, parts_ref):
    heads, kept, _ = x_ref.shape
    cores, columns, tokens, _ = parts_ref.shape
    rest = tokens - kept
    quarter = LANES // heads * columns
    lane = lax.broadcasted_iota(jnp.int32, (tokens, LANES), 1)
    for column in range(columns):
        parts = [jnp.zeros((tokens, LANES), jnp.float32)] * cores
        for group in range(heads // columns):
            block = x_ref[group * columns + column].astype(jnp.float32)
            for core in range(cores):
                home = group * quarter
                top = pltpu.roll(block, (home - core * quarter) % LANES, 1)
                bottom = pltpu.roll(block, (home - core * quarter - HEAD_DIM) % LANES, 1)[:rest]
                moved = jnp.concatenate([top, bottom], axis=0)
                inside = (lane >= home) & (lane < home + quarter)
                parts[core] = jnp.where(inside, moved, parts[core])
        for core in range(cores):
            part = parts[core].astype(jnp.bfloat16)
            parts_ref[core, column] = part
            rows_ref[core, :, column * LANES : (column + 1) * LANES] = part


def unpack_pair_kernel(x_ref, q_ref, k_ref):
    heads, tokens, _ = x_ref.shape
    low = low_lanes((tokens, LANES))
    for pair in range(heads // 2):
        first = x_ref[2 * pair].astype(jnp.float32)
        second = x_ref[2 * pair + 1].astype(jnp.float32)
        cols = slice(pair * LANES, (pair + 1) * LANES)
        q_ref[:, cols] = jnp.where(low, first, rolled(second)).astype(jnp.bfloat16)
        k_ref[:, cols] = jnp.where(low, rolled(first), second).astype(jnp.bfloat16)


def exchanged(x, axis):
    return lax.all_to_all(x, axis, split_axis=0, concat_axis=0, tiled=True)


def shifted(x, axis, step):
    count = lax.axis_size(axis)
    return lax.ppermute(x, axis, [(place, (place + step) % count) for place in range(count)])


def block_of(x, index):
    return lax.dynamic_index_in_dim(x, index, 0, keepdims=False)


def from_all(x, axis):
    return [x] + [shifted(x, axis, step) for step in range(1, lax.axis_size(axis))]


def sent_blocks(blocks, axis):
    count = lax.axis_size(axis)
    here = lax.axis_index(axis)
    own = block_of(blocks, here)
    return [own] + [
        shifted(block_of(blocks, (here + step) % count), axis, step) for step in range(1, count)
    ]


def placed(parts, axis):
    count = lax.axis_size(axis)
    here = lax.axis_index(axis)
    whole = jnp.zeros((count, *parts[0].shape), parts[0].dtype)
    for step, part in enumerate(parts):
        whole = lax.dynamic_update_index_in_dim(whole, part, (here - step) % count, 0)
    return whole.reshape(count * parts[0].shape[0], *parts[0].shape[1:])


def shaped(*shape, dtype=jnp.bfloat16):
    return jax.ShapeDtypeStruct(shape, dtype)


def shards(inputs, query_vectors, key_vectors, value_vectors, cotangent, gate_prefix, value_weight):
    planes = lax.axis_size("sp")
    cores, columns, lines = lax.axis_size("core"), lax.axis_size("x"), lax.axis_size("y")
    core = lax.axis_index("core")
    tokens, model = inputs.shape[1:]
    width = query_vectors.shape[2]
    heads = width // HEAD_DIM
    length = planes * tokens
    w_cols = value_weight.shape[1]
    weight_block = jnp.broadcast_to(value_weight.T, (planes, w_cols, model // planes))
    weight_block = exchanged(weight_block, "sp")
    weight_block = jnp.moveaxis(weight_block, 0, 1).reshape(w_cols, model)
    packed = pl.pallas_call(pack_kernel, out_shape=shaped(heads, tokens, 2 * LANES))(
        query_vectors[0], key_vectors[0], value_vectors[0], cotangent[0]
    )
    arrived = exchanged(packed, "sp")
    input_rows = jnp.concatenate(from_all(inputs[0], "x"), axis=0)
    input_rows = jnp.concatenate(from_all(input_rows, "core"), axis=0)
    weight_line = placed(from_all(weight_block, "y"), "y")
    weight_half = placed(from_all(weight_line, "x"), "x")
    weight_halves = from_all(weight_half, "core")
    kept = (tokens // 2 + 7) // 8 * 8
    pair_grad, value_grad = pl.pallas_call(
        attention_kernel,
        out_shape=(shaped(length, LANES), shaped(planes, kept, LANES)),
        scratch_shapes=[
            pltpu.VMEM((length, LANES), jnp.bfloat16),
            pltpu.VMEM((HEAD_DIM, length), jnp.bfloat16),
            pltpu.VMEM((length, LANES), jnp.float32),
            pltpu.VMEM((length, LANES), jnp.float32),
            pltpu.VMEM((length, LANES), jnp.float32),
            pltpu.VMEM((length, TILE), jnp.float32),
            pltpu.VMEM((length, TILE), jnp.float32),
        ],
    )(arrived.reshape(length, 2 * LANES), gate_prefix[0])
    value_back = exchanged(value_grad, "sp")
    pair_back = exchanged(pair_grad.reshape(planes, tokens, LANES), "sp")
    value_rows, value_parts = pl.pallas_call(
        unpack_value_kernel,
        out_shape=(shaped(cores, tokens, width // cores), shaped(cores, columns, tokens, LANES)),
    )(value_back)
    away = shifted(block_of(value_parts, 1 - core), "core", 1)
    both = jnp.concatenate([block_of(value_parts, core), away], axis=1)
    pieces = sent_blocks(both, "x")
    value_cols = jnp.concatenate(
        [piece[:tokens] for piece in pieces] + [piece[tokens:] for piece in pieces], axis=0
    )
    partial = lax.dot_general(
        value_cols, input_rows, (((0,), (0,)), ((), ())), preferred_element_type=jnp.float32
    ).astype(jnp.bfloat16)
    partial = sent_blocks(partial.reshape(lines, w_cols, model), "y")
    partial = sum(part.astype(jnp.float32) for part in partial).astype(jnp.bfloat16)
    partial = jnp.moveaxis(partial.reshape(w_cols, planes, model // planes), 1, 0)
    partial = exchanged(partial, "sp")
    weight_grad = partial.astype(jnp.float32).sum(axis=0).T
    query_grad, key_grad = pl.pallas_call(
        unpack_pair_kernel, out_shape=(shaped(tokens, width), shaped(tokens, width))
    )(pair_back)
    input_grad = sum(
        lax.dot_general(
            block_of(value_rows, place),
            half,
            (((1,), (0,)), ((), ())),
            preferred_element_type=jnp.float32,
        )
        for place, half in zip((core, 1 - core), weight_halves)
    ).astype(jnp.bfloat16)
    return (query_grad[None], key_grad[None], input_grad[None], weight_grad)


def solution(mesh):
    grid = Mesh(mesh.devices.reshape(-1, 4, 4, 2), ("sp", "y", "x", "core"))
    rows = P(("y", "x", "core"), "sp", None)
    weight = P("sp", ("y", "x", "core"))

    return jax.shard_map(
        shards,
        mesh=grid,
        in_specs=(rows,) * 6 + (weight,),
        out_specs=(rows, rows, rows, weight),
        check_vma=False,
    )
```

```python
import jax
import jax.numpy as jnp
from jax import lax
from jax.experimental import pallas as pl
from jax.experimental.pallas import tpu as pltpu
from jax.sharding import Mesh, PartitionSpec as P

HEAD_DIM = 64
LANES = 128
TILE = 256
FLOOR = -1e30


def rolled(x):
    return pltpu.roll(x, HEAD_DIM, 1)


def low_lanes(shape):
    return lax.broadcasted_iota(jnp.int32, shape, 1) < HEAD_DIM


def pack_kernel(q_ref, k_ref, v_ref, g_ref, out_ref):
    heads, tokens, _ = out_ref.shape
    low = low_lanes((tokens, LANES))
    for pair in range(heads // 2):
        cols = slice(pair * LANES, (pair + 1) * LANES)
        for first_ref, second_ref, lane in ((q_ref, k_ref, 0), (v_ref, g_ref, LANES)):
            first = first_ref[:, cols].astype(jnp.float32)
            second = second_ref[:, cols].astype(jnp.float32)
            out_ref[2 * pair, :, lane : lane + LANES] = jnp.where(
                low, first, rolled(second)
            ).astype(jnp.bfloat16)
            out_ref[2 * pair + 1, :, lane : lane + LANES] = jnp.where(
                low, rolled(first), second
            ).astype(jnp.bfloat16)


def dot_nt(a, b):
    return lax.dot_general(a, b, (((1,), (1,)), ((), ())), preferred_element_type=jnp.float32)


def dot_nn(a, b):
    return lax.dot_general(a, b, (((1,), (0,)), ((), ())), preferred_element_type=jnp.float32)


def folded(x, op):
    return op(x.reshape(x.shape[0] // 8, 8, x.shape[1]), axis=0)


def blocks_of(length):
    return [(base, min(TILE, length - base)) for base in range(0, length, TILE)]


def spread(x_ref, p_ref, kq_ref, pc_ref, acc_ref, kt_ref=None):
    for base, rows in blocks_of(x_ref.shape[0]):
        here = slice(base, base + rows)
        swapped = rolled(x_ref[here, :LANES].astype(jnp.float32))
        kq_ref[here] = swapped.astype(jnp.bfloat16)
        if kt_ref is not None:
            kt_ref[:, here] = swapped.T[:HEAD_DIM].astype(jnp.bfloat16)
        pc_ref[here] = jnp.broadcast_to(p_ref[:, here], (LANES, rows)).T
        acc_ref[here] = jnp.zeros((rows, LANES), jnp.float32)


def query_block(x_ref, here, low):
    wide = x_ref[here, :LANES].astype(jnp.float32)
    scaled = jnp.where(low, wide * HEAD_DIM**-0.5, 0.0).astype(jnp.bfloat16)
    return scaled, jnp.where(low, 0.0, rolled(wide)).astype(jnp.bfloat16)


def grad_block(x_ref, here, low):
    wide = rolled(x_ref[here, LANES:].astype(jnp.float32))
    return jnp.where(low, wide, 0.0).astype(jnp.bfloat16)


def score_tile(kq_ref, pc_ref, query_low, q_base, u_base, u_rows):
    q_rows = query_low.shape[0]
    shift = pc_ref[q_base : q_base + 1, :] - pc_ref[u_base : u_base + u_rows]
    shift = jnp.concatenate([shift] * (q_rows // LANES), axis=1)
    scores = dot_nt(kq_ref[u_base : u_base + u_rows], query_low) + shift
    if u_base != q_base:
        return scores
    place = lax.broadcasted_iota(jnp.int32, scores.shape, 0)
    seen = place <= lax.broadcasted_iota(jnp.int32, scores.shape, 1)
    return jnp.where(seen, scores, FLOOR)


def value_kernel(x_ref, p_ref, v_out_ref, peak_ref, share_ref, kq_ref, pc_ref, acc_ref, s_ref):
    length = x_ref.shape[0]
    blocks = blocks_of(length)
    spread(x_ref, p_ref, kq_ref, pc_ref, acc_ref)
    for index, (q_base, q_rows) in enumerate(blocks):
        q_here = slice(q_base, q_base + q_rows)
        low = low_lanes((q_rows, LANES))
        query_low, _ = query_block(x_ref, q_here, low)
        grad_low = grad_block(x_ref, q_here, low)
        peak = jnp.full((8, q_rows), FLOOR, jnp.float32)
        for u_base, u_rows in blocks[: index + 1]:
            scores = score_tile(kq_ref, pc_ref, query_low, q_base, u_base, u_rows)
            s_ref[u_base : u_base + u_rows, :q_rows] = scores
            peak = jnp.maximum(peak, folded(scores, jnp.max))
        peak = jnp.max(peak, axis=0, keepdims=True)
        total = jnp.zeros((8, q_rows), jnp.float32)
        for u_base, u_rows in blocks[: index + 1]:
            u_here = slice(u_base, u_base + u_rows)
            raised = jnp.exp(s_ref[u_here, :q_rows] - peak)
            s_ref[u_here, :q_rows] = raised
            total = total + folded(raised, jnp.sum)
        share = 1.0 / jnp.sum(total, axis=0, keepdims=True)
        peak_ref[:, q_here] = peak
        share_ref[:, q_here] = share
        for u_base, u_rows in blocks[: index + 1]:
            u_here = slice(u_base, u_base + u_rows)
            soft = s_ref[u_here, :q_rows] * share
            acc_ref[u_here] += dot_nn(soft.astype(jnp.bfloat16), grad_low)
    planes, kept, _ = v_out_ref.shape
    tokens = length // planes
    for plane in range(planes):
        base = plane * tokens
        first = acc_ref[base : base + kept]
        second = acc_ref[base + kept : base + tokens]
        second = jnp.concatenate([second, first[: 2 * kept - tokens]], axis=0)
        v_out_ref[plane] = jnp.where(low_lanes(first.shape), first, rolled(second)).astype(
            jnp.bfloat16
        )


def pair_kernel(
    x_ref, p_ref, peak_ref, share_ref, qk_ref, kq_ref, kt_ref, pc_ref, acc_ref, s_ref, d_ref
):
    blocks = blocks_of(x_ref.shape[0])
    scale = HEAD_DIM**-0.5
    spread(x_ref, p_ref, kq_ref, pc_ref, acc_ref, kt_ref)
    for index, (q_base, q_rows) in enumerate(blocks):
        q_here = slice(q_base, q_base + q_rows)
        low = low_lanes((q_rows, LANES))
        query_low, query_high = query_block(x_ref, q_here, low)
        grad_low = grad_block(x_ref, q_here, low)
        peak = peak_ref[:, q_here]
        share = share_ref[:, q_here]
        term = jnp.zeros((8, q_rows), jnp.float32)
        for u_base, u_rows in blocks[: index + 1]:
            u_here = slice(u_base, u_base + u_rows)
            scores = score_tile(kq_ref, pc_ref, query_low, q_base, u_base, u_rows)
            soft = jnp.exp(scores - peak) * share
            s_ref[u_here, :q_rows] = soft
            soft_grad = dot_nt(x_ref[u_here, LANES:], grad_low)
            d_ref[u_here, :q_rows] = soft_grad
            term = term + folded(soft * soft_grad, jnp.sum)
        term = jnp.sum(term, axis=0, keepdims=True)
        query_grad = jnp.zeros((HEAD_DIM, q_rows), jnp.float32)
        for u_base, u_rows in blocks[: index + 1]:
            u_here = slice(u_base, u_base + u_rows)
            score_low = (s_ref[u_here, :q_rows] * (d_ref[u_here, :q_rows] - term)).astype(
                jnp.bfloat16
            )
            acc_ref[u_here] += dot_nn(score_low, query_high)
            query_grad = query_grad + dot_nn(kt_ref[:, u_here], score_low)
        query_grad = jnp.concatenate([query_grad, jnp.zeros_like(query_grad)], axis=0)
        acc_ref[q_here] += query_grad.T
    for base, rows in blocks:
        here = slice(base, base + rows)
        qk_ref[here] = (acc_ref[here] * scale).astype(jnp.bfloat16)


def unpack_value_kernel(place_ref, x_ref, rows_ref, mine_ref, away_ref):
    heads, kept, _ = x_ref.shape
    cores = rows_ref.shape[0]
    columns, tokens, _ = mine_ref.shape
    rest = tokens - kept
    quarter = LANES // heads * columns
    lane = lax.broadcasted_iota(jnp.int32, (tokens, LANES), 1)
    first_core = place_ref[0] == 0
    for column in range(columns):
        step = (column + columns - place_ref[1]) % columns
        parts = [jnp.zeros((tokens, LANES), jnp.float32)] * cores
        for group in range(heads // columns):
            block = x_ref[group * columns + column].astype(jnp.float32)
            for core in range(cores):
                home = group * quarter
                top = pltpu.roll(block, (home - core * quarter) % LANES, 1)
                bottom = pltpu.roll(block, (home - core * quarter - HEAD_DIM) % LANES, 1)[:rest]
                moved = jnp.concatenate([top, bottom], axis=0)
                inside = (lane >= home) & (lane < home + quarter)
                parts[core] = jnp.where(inside, moved, parts[core])
        mine = jnp.where(first_core, parts[0], parts[1]).astype(jnp.bfloat16)
        away = jnp.where(first_core, parts[1], parts[0]).astype(jnp.bfloat16)
        mine_ref[step] = mine
        away_ref[step] = away
        rows_ref[0, :, column * LANES : (column + 1) * LANES] = mine
        rows_ref[1, :, column * LANES : (column + 1) * LANES] = away


def unpack_pair_kernel(x_ref, q_ref, k_ref):
    heads, tokens, _ = x_ref.shape
    low = low_lanes((tokens, LANES))
    for pair in range(heads // 2):
        first = x_ref[2 * pair].astype(jnp.float32)
        second = x_ref[2 * pair + 1].astype(jnp.float32)
        cols = slice(pair * LANES, (pair + 1) * LANES)
        q_ref[:, cols] = jnp.where(low, first, rolled(second)).astype(jnp.bfloat16)
        k_ref[:, cols] = jnp.where(low, rolled(first), second).astype(jnp.bfloat16)


def exchanged(x, axis):
    return lax.all_to_all(x, axis, split_axis=0, concat_axis=0, tiled=True)


def shifted(x, axis, step):
    count = lax.axis_size(axis)
    return lax.ppermute(x, axis, [(place, (place + step) % count) for place in range(count)])


def block_of(x, index):
    return lax.dynamic_index_in_dim(x, index, 0, keepdims=False)


def from_all(x, axis):
    return [x] + [shifted(x, axis, step) for step in range(1, lax.axis_size(axis))]


def sent_blocks(blocks, axis):
    count = lax.axis_size(axis)
    here = lax.axis_index(axis)
    own = block_of(blocks, here)
    return [own] + [
        shifted(block_of(blocks, (here + step) % count), axis, step) for step in range(1, count)
    ]


def placed(parts, axis):
    count = lax.axis_size(axis)
    here = lax.axis_index(axis)
    whole = jnp.zeros((count, *parts[0].shape), parts[0].dtype)
    for step, part in enumerate(parts):
        whole = lax.dynamic_update_index_in_dim(whole, part, (here - step) % count, 0)
    return whole.reshape(count * parts[0].shape[0], *parts[0].shape[1:])


def shaped(*shape, dtype=jnp.bfloat16):
    return jax.ShapeDtypeStruct(shape, dtype)


def shards(inputs, query_vectors, key_vectors, value_vectors, cotangent, gate_prefix, value_weight):
    planes = lax.axis_size("sp")
    cores, columns, lines = lax.axis_size("core"), lax.axis_size("x"), lax.axis_size("y")
    core = lax.axis_index("core")
    tokens, model = inputs.shape[1:]
    width = query_vectors.shape[2]
    heads = width // HEAD_DIM
    length = planes * tokens
    w_cols = value_weight.shape[1]
    weight_block = jnp.broadcast_to(value_weight.T, (planes, w_cols, model // planes))
    weight_block = exchanged(weight_block, "sp")
    weight_block = jnp.moveaxis(weight_block, 0, 1).reshape(w_cols, model)
    packed = pl.pallas_call(pack_kernel, out_shape=shaped(heads, tokens, 2 * LANES))(
        query_vectors[0], key_vectors[0], value_vectors[0], cotangent[0]
    )
    arrived = exchanged(packed, "sp")
    own_rows = jnp.stack(from_all(inputs[0], "x"))
    input_rows = jnp.stack([own_rows, shifted(own_rows, "core", 1)], axis=1)
    input_rows = input_rows.reshape(cores * columns * tokens, model)
    weight_line = placed(from_all(weight_block, "y"), "y")
    weight_half = placed(from_all(weight_line, "x"), "x")
    weight_halves = from_all(weight_half, "core")
    kept = (tokens // 2 + 7) // 8 * 8
    arrived, input_rows = lax.optimization_barrier((arrived, input_rows))
    sequence = arrived.reshape(length, 2 * LANES)
    wide, tile = pltpu.VMEM((length, LANES), jnp.float32), pltpu.VMEM((length, TILE), jnp.float32)
    row = shaped(1, length, dtype=jnp.float32)
    value_grad, peak, share = pl.pallas_call(
        value_kernel,
        out_shape=(shaped(planes, kept, LANES), row, row),
        scratch_shapes=[pltpu.VMEM((length, LANES), jnp.bfloat16), wide, wide, tile],
    )(sequence, gate_prefix[0])
    value_back = exchanged(value_grad, "sp")
    pair_grad = pl.pallas_call(
        pair_kernel,
        out_shape=shaped(length, LANES),
        scratch_shapes=[
            pltpu.VMEM((length, LANES), jnp.bfloat16),
            pltpu.VMEM((HEAD_DIM, length), jnp.bfloat16),
            wide,
            wide,
            tile,
            tile,
        ],
    )(sequence, gate_prefix[0], peak, share)
    pair_back = exchanged(pair_grad.reshape(planes, tokens, LANES), "sp")
    place = jnp.stack([core, lax.axis_index("x")]).astype(jnp.int32)
    block = shaped(columns, tokens, LANES)
    whole = pl.BlockSpec(memory_space=pltpu.VMEM)
    value_rows, mine, away = pl.pallas_call(
        unpack_value_kernel,
        out_shape=(shaped(cores, tokens, width // cores), block, block),
        in_specs=[pl.BlockSpec(memory_space=pltpu.SMEM), whole],
    )(place, value_back)
    both = jnp.stack([mine, shifted(away, "core", 1)], axis=1)
    pieces = [both[0]] + [shifted(both[step], "x", step) for step in range(1, columns)]
    value_cols = jnp.stack(pieces).reshape(columns * cores * tokens, LANES)
    partial = lax.dot_general(
        value_cols, input_rows, (((0,), (0,)), ((), ())), preferred_element_type=jnp.float32
    ).astype(jnp.bfloat16)
    partial = sent_blocks(partial.reshape(lines, w_cols, model), "y")
    partial = sum(part.astype(jnp.float32) for part in partial).astype(jnp.bfloat16)
    partial = jnp.moveaxis(partial.reshape(w_cols, planes, model // planes), 1, 0)
    partial = exchanged(partial, "sp")
    weight_grad = partial.astype(jnp.float32).sum(axis=0).T
    query_grad, key_grad = pl.pallas_call(
        unpack_pair_kernel, out_shape=(shaped(tokens, width), shaped(tokens, width))
    )(pair_back)
    input_grad = sum(
        lax.dot_general(
            value_rows[place],
            half,
            (((1,), (0,)), ((), ())),
            preferred_element_type=jnp.float32,
        )
        for place, half in enumerate(weight_halves)
    ).astype(jnp.bfloat16)
    return (query_grad[None], key_grad[None], input_grad[None], weight_grad)


def solution(mesh):
    grid = Mesh(mesh.devices.reshape(-1, 4, 4, 2), ("sp", "y", "x", "core"))
    rows = P(("y", "x", "core"), "sp", None)
    weight = P("sp", ("y", "x", "core"))

    return jax.shard_map(
        shards,
        mesh=grid,
        in_specs=(rows,) * 6 + (weight,),
        out_specs=(rows, rows, rows, weight),
        check_vma=False,
    )
```

```python
import jax
import jax.numpy as jnp
from jax import lax
from jax.experimental import pallas as pl
from jax.experimental.pallas import tpu as pltpu
from jax.sharding import Mesh, PartitionSpec as P

HEAD_DIM = 64
LANES = 128
TILE = 256
FLOOR = -1e30


def rolled(x):
    return pltpu.roll(x, HEAD_DIM, 1)


def low_lanes(shape):
    return lax.broadcasted_iota(jnp.int32, shape, 1) < HEAD_DIM


def pack_kernel(q_ref, k_ref, v_ref, g_ref, out_ref):
    heads, tokens, _ = out_ref.shape
    low = low_lanes((tokens, LANES))
    for pair in range(heads // 2):
        cols = slice(pair * LANES, (pair + 1) * LANES)
        for first_ref, second_ref, lane in ((q_ref, k_ref, 0), (v_ref, g_ref, LANES)):
            first = first_ref[:, cols].astype(jnp.float32)
            second = second_ref[:, cols].astype(jnp.float32)
            out_ref[2 * pair, :, lane : lane + LANES] = jnp.where(
                low, first, rolled(second)
            ).astype(jnp.bfloat16)
            out_ref[2 * pair + 1, :, lane : lane + LANES] = jnp.where(
                low, rolled(first), second
            ).astype(jnp.bfloat16)


def dot_nt(a, b):
    return lax.dot_general(a, b, (((1,), (1,)), ((), ())), preferred_element_type=jnp.float32)


def dot_nn(a, b):
    return lax.dot_general(a, b, (((1,), (0,)), ((), ())), preferred_element_type=jnp.float32)


def folded(x, op):
    return op(x.reshape(x.shape[0] // 8, 8, x.shape[1]), axis=0)


def blocks_of(length):
    return [(base, min(TILE, length - base)) for base in range(0, length, TILE)]


def spread(x_ref, p_ref, kq_ref, pc_ref, acc_ref, kt_ref=None):
    for base, rows in blocks_of(x_ref.shape[0]):
        here = slice(base, base + rows)
        swapped = rolled(x_ref[here, :LANES].astype(jnp.float32))
        kq_ref[here] = swapped.astype(jnp.bfloat16)
        if kt_ref is not None:
            kt_ref[:, here] = swapped.T[:HEAD_DIM].astype(jnp.bfloat16)
        pc_ref[here] = jnp.broadcast_to(p_ref[:, here], (LANES, rows)).T
        acc_ref[here] = jnp.zeros((rows, LANES), jnp.float32)


def query_block(x_ref, here, low):
    wide = x_ref[here, :LANES].astype(jnp.float32)
    scaled = jnp.where(low, wide * HEAD_DIM**-0.5, 0.0).astype(jnp.bfloat16)
    return scaled, jnp.where(low, 0.0, rolled(wide)).astype(jnp.bfloat16)


def grad_block(x_ref, here, low):
    wide = rolled(x_ref[here, LANES:].astype(jnp.float32))
    return jnp.where(low, wide, 0.0).astype(jnp.bfloat16)


def score_tile(kq_ref, pc_ref, query_low, q_base, u_base, u_rows):
    q_rows = query_low.shape[0]
    shift = pc_ref[q_base : q_base + 1, :] - pc_ref[u_base : u_base + u_rows]
    shift = jnp.concatenate([shift] * (q_rows // LANES), axis=1)
    scores = dot_nt(kq_ref[u_base : u_base + u_rows], query_low) + shift
    if u_base != q_base:
        return scores
    place = lax.broadcasted_iota(jnp.int32, scores.shape, 0)
    seen = place <= lax.broadcasted_iota(jnp.int32, scores.shape, 1)
    return jnp.where(seen, scores, FLOOR)


def value_kernel(x_ref, p_ref, v_out_ref, peak_ref, share_ref, kq_ref, pc_ref, acc_ref, s_ref):
    length = x_ref.shape[0]
    blocks = blocks_of(length)
    spread(x_ref, p_ref, kq_ref, pc_ref, acc_ref)
    for index, (q_base, q_rows) in enumerate(blocks):
        q_here = slice(q_base, q_base + q_rows)
        low = low_lanes((q_rows, LANES))
        query_low, _ = query_block(x_ref, q_here, low)
        grad_low = grad_block(x_ref, q_here, low)
        peak = jnp.full((8, q_rows), FLOOR, jnp.float32)
        for u_base, u_rows in blocks[: index + 1]:
            scores = score_tile(kq_ref, pc_ref, query_low, q_base, u_base, u_rows)
            s_ref[u_base : u_base + u_rows, :q_rows] = scores
            peak = jnp.maximum(peak, folded(scores, jnp.max))
        peak = jnp.max(peak, axis=0, keepdims=True)
        total = jnp.zeros((8, q_rows), jnp.float32)
        for u_base, u_rows in blocks[: index + 1]:
            u_here = slice(u_base, u_base + u_rows)
            raised = jnp.exp(s_ref[u_here, :q_rows] - peak)
            s_ref[u_here, :q_rows] = raised
            total = total + folded(raised, jnp.sum)
        share = 1.0 / jnp.sum(total, axis=0, keepdims=True)
        peak_ref[:, q_here] = peak
        share_ref[:, q_here] = share
        for u_base, u_rows in blocks[: index + 1]:
            u_here = slice(u_base, u_base + u_rows)
            soft = s_ref[u_here, :q_rows] * share
            acc_ref[u_here] += dot_nn(soft.astype(jnp.bfloat16), grad_low)
    planes, kept, _ = v_out_ref.shape
    tokens = length // planes
    for plane in range(planes):
        base = plane * tokens
        first = acc_ref[base : base + kept]
        second = acc_ref[base + kept : base + tokens]
        second = jnp.concatenate([second, first[: 2 * kept - tokens]], axis=0)
        v_out_ref[plane] = jnp.where(low_lanes(first.shape), first, rolled(second)).astype(
            jnp.bfloat16
        )


def pair_kernel(
    x_ref, p_ref, peak_ref, share_ref, qk_ref, kq_ref, kt_ref, pc_ref, acc_ref, s_ref, d_ref
):
    blocks = blocks_of(x_ref.shape[0])
    scale = HEAD_DIM**-0.5
    spread(x_ref, p_ref, kq_ref, pc_ref, acc_ref, kt_ref)
    for index, (q_base, q_rows) in enumerate(blocks):
        q_here = slice(q_base, q_base + q_rows)
        low = low_lanes((q_rows, LANES))
        query_low, query_high = query_block(x_ref, q_here, low)
        grad_low = grad_block(x_ref, q_here, low)
        peak = peak_ref[:, q_here]
        share = share_ref[:, q_here]
        term = jnp.zeros((8, q_rows), jnp.float32)
        for u_base, u_rows in blocks[: index + 1]:
            u_here = slice(u_base, u_base + u_rows)
            scores = score_tile(kq_ref, pc_ref, query_low, q_base, u_base, u_rows)
            soft = jnp.exp(scores - peak) * share
            s_ref[u_here, :q_rows] = soft
            soft_grad = dot_nt(x_ref[u_here, LANES:], grad_low)
            d_ref[u_here, :q_rows] = soft_grad
            term = term + folded(soft * soft_grad, jnp.sum)
        term = jnp.sum(term, axis=0, keepdims=True)
        query_grad = jnp.zeros((HEAD_DIM, q_rows), jnp.float32)
        for u_base, u_rows in blocks[: index + 1]:
            u_here = slice(u_base, u_base + u_rows)
            score_low = (s_ref[u_here, :q_rows] * (d_ref[u_here, :q_rows] - term)).astype(
                jnp.bfloat16
            )
            acc_ref[u_here] += dot_nn(score_low, query_high)
            query_grad = query_grad + dot_nn(kt_ref[:, u_here], score_low)
        query_grad = jnp.concatenate([query_grad, jnp.zeros_like(query_grad)], axis=0)
        acc_ref[q_here] += query_grad.T
    for base, rows in blocks:
        here = slice(base, base + rows)
        qk_ref[here] = (acc_ref[here] * scale).astype(jnp.bfloat16)


def unpack_value_kernel(place_ref, x_ref, mine_ref, away_ref):
    heads, kept, _ = x_ref.shape
    columns, tokens, _ = mine_ref.shape
    rest = tokens - kept
    cores = HEAD_DIM * columns // LANES
    quarter = HEAD_DIM // cores
    lane = lax.broadcasted_iota(jnp.int32, (tokens, LANES), 1)
    first_core = place_ref[0] == 0
    for column in range(columns):
        step = (column + columns - place_ref[1]) % columns
        parts = [jnp.zeros((tokens, LANES), jnp.float32)] * cores
        for group in range(heads // columns):
            block = x_ref[group * columns + column].astype(jnp.float32)
            for core in range(cores):
                home = group * quarter
                top = pltpu.roll(block, (home - core * quarter) % LANES, 1)
                bottom = pltpu.roll(block, (home - core * quarter - HEAD_DIM) % LANES, 1)[:rest]
                moved = jnp.concatenate([top, bottom], axis=0)
                inside = (lane >= home) & (lane < home + quarter)
                parts[core] = jnp.where(inside, moved, parts[core])
        mine_ref[step] = jnp.where(first_core, parts[0], parts[1]).astype(jnp.bfloat16)
        away_ref[step] = jnp.where(first_core, parts[1], parts[0]).astype(jnp.bfloat16)


def weight_open_kernel(x_ref, out_ref):
    for plane in range(x_ref.shape[0]):
        out_ref[:, plane * LANES : (plane + 1) * LANES] = x_ref[plane]


def weight_line_kernel(place_ref, *refs):
    pieces, out_ref = refs[:-1], refs[-1]
    lines = out_ref.shape[0]
    for step, piece_ref in enumerate(pieces):
        out_ref[(place_ref[2] + lines - step) % lines] = piece_ref[...]


def stack_kernel(*refs):
    for step, piece_ref in enumerate(refs[:-1]):
        refs[-1][step] = piece_ref[...]


def dot_tn(a, b):
    return lax.dot_general(a, b, (((0,), (0,)), ((), ())), preferred_element_type=jnp.float32)


def product_kernel(place_ref, own_ref, other_ref, *refs):
    columns = own_ref.shape[0]
    pieces, (block_ref,) = refs[:columns], refs[-1:]
    outs = refs[columns:-1]
    lines, w_cols, model = block_ref.shape
    width = 4 * LANES
    own = jnp.concatenate([piece[0] for piece in pieces], axis=0)
    other = jnp.concatenate([piece[1] for piece in pieces], axis=0)
    rows = own.shape[0]
    for base in range(0, model, width):
        cols = slice(base, base + width)
        total = dot_tn(own, own_ref[:, :, cols].reshape(rows, width))
        total = total + dot_tn(other, other_ref[:, :, cols].reshape(rows, width))
        block_ref[:, :, cols] = total.astype(jnp.bfloat16).reshape(lines, w_cols, width)
    for step, out_ref in enumerate(outs):
        out_ref[...] = block_ref[(place_ref[2] + step) % lines]


def input_grad_kernel(both_ref, *refs):
    columns, cores, tokens, _ = both_ref.shape
    weights, (mine_ref, away_ref) = refs[:columns], refs[columns:]
    width = 4 * LANES
    for base in range(0, mine_ref.shape[1], width):
        cols = slice(base, base + width)
        total = jnp.zeros((cores * tokens, width), jnp.float32)
        for step in range(columns):
            total = total + dot_nn(
                both_ref[step].reshape(cores * tokens, LANES),
                weights[(columns - step) % columns][:, cols],
            )
        mine_ref[:, cols] = total[:tokens]
        away_ref[:, cols] = total[tokens:].astype(jnp.bfloat16)


def unpack_pair_kernel(x_ref, q_ref, k_ref):
    heads, tokens, _ = x_ref.shape
    low = low_lanes((tokens, LANES))
    for pair in range(heads // 2):
        first = x_ref[2 * pair].astype(jnp.float32)
        second = x_ref[2 * pair + 1].astype(jnp.float32)
        cols = slice(pair * LANES, (pair + 1) * LANES)
        q_ref[:, cols] = jnp.where(low, first, rolled(second)).astype(jnp.bfloat16)
        k_ref[:, cols] = jnp.where(low, rolled(first), second).astype(jnp.bfloat16)


def exchanged(x, axis):
    return lax.all_to_all(x, axis, split_axis=0, concat_axis=0, tiled=True)


def shifted(x, axis, step):
    count = lax.axis_size(axis)
    return lax.ppermute(x, axis, [(place, (place + step) % count) for place in range(count)])


def from_all(x, axis):
    return [x] + [shifted(x, axis, step) for step in range(1, lax.axis_size(axis))]


def near(x):
    return pltpu.with_memory_space_constraint(x, pltpu.VMEM)


def shaped(*shape, dtype=jnp.bfloat16):
    return jax.ShapeDtypeStruct(shape, dtype)


def shards(inputs, query_vectors, key_vectors, value_vectors, cotangent, gate_prefix, value_weight):
    planes = lax.axis_size("sp")
    columns, lines = lax.axis_size("x"), lax.axis_size("y")
    core = lax.axis_index("core")
    tokens, model = inputs.shape[1:]
    width = query_vectors.shape[2]
    heads = width // HEAD_DIM
    length = planes * tokens
    w_cols = value_weight.shape[1]
    weight_block = jnp.broadcast_to(value_weight.T, (planes, w_cols, model // planes))
    weight_block = exchanged(weight_block, "sp")
    place = jnp.stack([core, lax.axis_index("x"), lax.axis_index("y")]).astype(jnp.int32)
    small, whole = pl.BlockSpec(memory_space=pltpu.SMEM), pl.BlockSpec(memory_space=pltpu.VMEM)
    weight_block = pl.pallas_call(weight_open_kernel, out_shape=shaped(w_cols, model))(
        near(weight_block)
    )
    packed = pl.pallas_call(pack_kernel, out_shape=shaped(heads, tokens, 2 * LANES))(
        query_vectors[0], key_vectors[0], value_vectors[0], cotangent[0]
    )
    arrived = exchanged(packed, "sp")
    own_rows = pl.pallas_call(stack_kernel, out_shape=shaped(columns, tokens, model))(
        inputs[0], *map(near, from_all(inputs[0], "x")[1:])
    )
    other_rows = shifted(own_rows, "core", 1)
    weight_line = pl.pallas_call(
        weight_line_kernel,
        out_shape=shaped(lines, w_cols, model),
        in_specs=[small] + [whole] * lines,
    )(place, weight_block, *map(near, from_all(weight_block, "y")[1:])).reshape(lines * w_cols, model)
    weight_pieces = from_all(weight_line, "x")
    kept = (tokens // 2 + 7) // 8 * 8
    sequence = near(arrived.reshape(length, 2 * LANES))
    wide, tile = pltpu.VMEM((length, LANES), jnp.float32), pltpu.VMEM((length, TILE), jnp.float32)
    row = shaped(1, length, dtype=jnp.float32)
    value_grad, peak, share = pl.pallas_call(
        value_kernel,
        out_shape=(shaped(planes, kept, LANES), row, row),
        scratch_shapes=[pltpu.VMEM((length, LANES), jnp.bfloat16), wide, wide, tile],
    )(sequence, gate_prefix[0])
    value_back = exchanged(value_grad, "sp")
    pair_grad = pl.pallas_call(
        pair_kernel,
        out_shape=shaped(length, LANES),
        scratch_shapes=[
            pltpu.VMEM((length, LANES), jnp.bfloat16),
            pltpu.VMEM((HEAD_DIM, length), jnp.bfloat16),
            wide,
            wide,
            tile,
            tile,
        ],
    )(sequence, gate_prefix[0], peak, share)
    pair_back = exchanged(pair_grad.reshape(planes, tokens, LANES), "sp")
    block = shaped(columns, tokens, LANES)
    mine, away = pl.pallas_call(
        unpack_value_kernel, out_shape=(block, block), in_specs=[small, whole]
    )(place, near(value_back))
    both = jnp.stack([mine, shifted(away, "core", 1)], axis=1)
    pieces = [both[0]] + [shifted(both[step], "x", step) for step in range(1, columns)]
    partial = pl.pallas_call(
        product_kernel,
        out_shape=(shaped(w_cols, model),) * lines,
        in_specs=[small] + [whole] * (2 + columns),
        scratch_shapes=[pltpu.VMEM((lines, w_cols, model), jnp.bfloat16)],
    )(place, own_rows, near(other_rows), *map(near, pieces))
    partial = [partial[0]] + [shifted(partial[step], "y", step) for step in range(1, lines)]
    partial = sum(part.astype(jnp.float32) for part in partial).astype(jnp.bfloat16)
    partial = jnp.moveaxis(partial.reshape(w_cols, planes, model // planes), 1, 0)
    partial = exchanged(partial, "sp")
    weight_grad = partial.astype(jnp.float32).sum(axis=0).T
    query_grad, key_grad = pl.pallas_call(
        unpack_pair_kernel, out_shape=(shaped(tokens, width), shaped(tokens, width))
    )(near(pair_back))
    kept_part, sent_part = pl.pallas_call(
        input_grad_kernel,
        out_shape=(shaped(tokens, model, dtype=jnp.float32), shaped(tokens, model)),
    )(both, *weight_pieces)
    input_grad = (kept_part + shifted(sent_part, "core", 1)).astype(jnp.bfloat16)
    return (query_grad[None], key_grad[None], input_grad[None], weight_grad)


def solution(mesh):
    grid = Mesh(mesh.devices.reshape(-1, 4, 4, 2), ("sp", "y", "x", "core"))
    rows = P(("y", "x", "core"), "sp", None)
    weight = P("sp", ("y", "x", "core"))

    return jax.shard_map(
        shards,
        mesh=grid,
        in_specs=(rows,) * 6 + (weight,),
        out_specs=(rows, rows, rows, weight),
        check_vma=False,
    )
```

```python
import jax
import jax.numpy as jnp
from jax import lax
from jax.experimental import pallas as pl
from jax.experimental.pallas import tpu as pltpu
from jax.sharding import Mesh, PartitionSpec as P

HEAD_DIM = 64
LANES = 128
TILE = 256
FLOOR = -1e30


def rolled(x):
    return pltpu.roll(x, HEAD_DIM, 1)


def low_lanes(shape):
    return lax.broadcasted_iota(jnp.int32, shape, 1) < HEAD_DIM


def pack_kernel(q_ref, k_ref, v_ref, g_ref, out_ref):
    heads, tokens, _ = out_ref.shape
    low = low_lanes((tokens, LANES))
    for pair in range(heads // 2):
        cols = slice(pair * LANES, (pair + 1) * LANES)
        for first_ref, second_ref, lane in ((q_ref, k_ref, 0), (v_ref, g_ref, LANES)):
            first = first_ref[:, cols].astype(jnp.float32)
            second = second_ref[:, cols].astype(jnp.float32)
            out_ref[2 * pair, :, lane : lane + LANES] = jnp.where(
                low, first, rolled(second)
            ).astype(jnp.bfloat16)
            out_ref[2 * pair + 1, :, lane : lane + LANES] = jnp.where(
                low, rolled(first), second
            ).astype(jnp.bfloat16)


def dot_nt(a, b):
    return lax.dot_general(a, b, (((1,), (1,)), ((), ())), preferred_element_type=jnp.float32)


def dot_nn(a, b):
    return lax.dot_general(a, b, (((1,), (0,)), ((), ())), preferred_element_type=jnp.float32)


def folded(x, op):
    return op(x.reshape(x.shape[0] // 8, 8, x.shape[1]), axis=0)


def blocks_of(length):
    return [(base, min(TILE, length - base)) for base in range(0, length, TILE)]


def spread(x_ref, p_ref, kq_ref, pc_ref, acc_ref, kt_ref=None):
    for base, rows in blocks_of(x_ref.shape[0]):
        here = slice(base, base + rows)
        swapped = rolled(x_ref[here, :LANES].astype(jnp.float32))
        kq_ref[here] = swapped.astype(jnp.bfloat16)
        if kt_ref is not None:
            kt_ref[:, here] = swapped.T[:HEAD_DIM].astype(jnp.bfloat16)
        pc_ref[here] = jnp.broadcast_to(p_ref[:, here], (LANES, rows)).T
        acc_ref[here] = jnp.zeros((rows, LANES), jnp.float32)


def query_block(x_ref, here, low):
    wide = x_ref[here, :LANES].astype(jnp.float32)
    scaled = jnp.where(low, wide * HEAD_DIM**-0.5, 0.0).astype(jnp.bfloat16)
    return scaled, jnp.where(low, 0.0, rolled(wide)).astype(jnp.bfloat16)


def grad_block(x_ref, here, low):
    wide = rolled(x_ref[here, LANES:].astype(jnp.float32))
    return jnp.where(low, wide, 0.0).astype(jnp.bfloat16)


def score_tile(kq_ref, pc_ref, query_low, q_base, u_base, u_rows):
    q_rows = query_low.shape[0]
    shift = pc_ref[q_base : q_base + 1, :] - pc_ref[u_base : u_base + u_rows]
    shift = jnp.concatenate([shift] * (q_rows // LANES), axis=1)
    scores = dot_nt(kq_ref[u_base : u_base + u_rows], query_low) + shift
    if u_base != q_base:
        return scores
    place = lax.broadcasted_iota(jnp.int32, scores.shape, 0)
    seen = place <= lax.broadcasted_iota(jnp.int32, scores.shape, 1)
    return jnp.where(seen, scores, FLOOR)


def value_kernel(x_ref, p_ref, v_out_ref, peak_ref, share_ref, kq_ref, pc_ref, acc_ref, s_ref):
    length = x_ref.shape[0]
    blocks = blocks_of(length)
    spread(x_ref, p_ref, kq_ref, pc_ref, acc_ref)
    for index, (q_base, q_rows) in enumerate(blocks):
        q_here = slice(q_base, q_base + q_rows)
        low = low_lanes((q_rows, LANES))
        query_low, _ = query_block(x_ref, q_here, low)
        grad_low = grad_block(x_ref, q_here, low)
        peak = jnp.full((8, q_rows), FLOOR, jnp.float32)
        for u_base, u_rows in blocks[: index + 1]:
            scores = score_tile(kq_ref, pc_ref, query_low, q_base, u_base, u_rows)
            s_ref[u_base : u_base + u_rows, :q_rows] = scores
            peak = jnp.maximum(peak, folded(scores, jnp.max))
        peak = jnp.max(peak, axis=0, keepdims=True)
        total = jnp.zeros((8, q_rows), jnp.float32)
        for u_base, u_rows in blocks[: index + 1]:
            u_here = slice(u_base, u_base + u_rows)
            raised = jnp.exp(s_ref[u_here, :q_rows] - peak)
            s_ref[u_here, :q_rows] = raised
            total = total + folded(raised, jnp.sum)
        share = 1.0 / jnp.sum(total, axis=0, keepdims=True)
        peak_ref[:, q_here] = peak
        share_ref[:, q_here] = share
        for u_base, u_rows in blocks[: index + 1]:
            u_here = slice(u_base, u_base + u_rows)
            soft = s_ref[u_here, :q_rows] * share
            acc_ref[u_here] += dot_nn(soft.astype(jnp.bfloat16), grad_low)
    planes, kept, _ = v_out_ref.shape
    tokens = length // planes
    for plane in range(planes):
        base = plane * tokens
        first = acc_ref[base : base + kept]
        second = acc_ref[base + kept : base + tokens]
        second = jnp.concatenate([second, first[: 2 * kept - tokens]], axis=0)
        v_out_ref[plane] = jnp.where(low_lanes(first.shape), first, rolled(second)).astype(
            jnp.bfloat16
        )


def pair_kernel(
    x_ref, p_ref, peak_ref, share_ref, qk_ref, kq_ref, kt_ref, pc_ref, acc_ref, s_ref, d_ref
):
    blocks = blocks_of(x_ref.shape[0])
    scale = HEAD_DIM**-0.5
    spread(x_ref, p_ref, kq_ref, pc_ref, acc_ref, kt_ref)
    for index, (q_base, q_rows) in enumerate(blocks):
        q_here = slice(q_base, q_base + q_rows)
        low = low_lanes((q_rows, LANES))
        query_low, query_high = query_block(x_ref, q_here, low)
        grad_low = grad_block(x_ref, q_here, low)
        peak = peak_ref[:, q_here]
        share = share_ref[:, q_here]
        term = jnp.zeros((8, q_rows), jnp.float32)
        for u_base, u_rows in blocks[: index + 1]:
            u_here = slice(u_base, u_base + u_rows)
            scores = score_tile(kq_ref, pc_ref, query_low, q_base, u_base, u_rows)
            soft = jnp.exp(scores - peak) * share
            s_ref[u_here, :q_rows] = soft
            soft_grad = dot_nt(x_ref[u_here, LANES:], grad_low)
            d_ref[u_here, :q_rows] = soft_grad
            term = term + folded(soft * soft_grad, jnp.sum)
        term = jnp.sum(term, axis=0, keepdims=True)
        query_grad = jnp.zeros((HEAD_DIM, q_rows), jnp.float32)
        for u_base, u_rows in blocks[: index + 1]:
            u_here = slice(u_base, u_base + u_rows)
            score_low = (s_ref[u_here, :q_rows] * (d_ref[u_here, :q_rows] - term)).astype(
                jnp.bfloat16
            )
            acc_ref[u_here] += dot_nn(score_low, query_high)
            query_grad = query_grad + dot_nn(kt_ref[:, u_here], score_low)
        query_grad = jnp.concatenate([query_grad, jnp.zeros_like(query_grad)], axis=0)
        acc_ref[q_here] += query_grad.T
    for base, rows in blocks:
        here = slice(base, base + rows)
        qk_ref[here] = (acc_ref[here] * scale).astype(jnp.bfloat16)


def unpack_value_kernel(place_ref, x_ref, mine_ref, away_ref):
    heads, kept, _ = x_ref.shape
    columns, tokens, _ = mine_ref.shape
    rest = tokens - kept
    cores = HEAD_DIM * columns // LANES
    quarter = HEAD_DIM // cores
    lane = lax.broadcasted_iota(jnp.int32, (tokens, LANES), 1)
    first_core = place_ref[0] == 0
    for column in range(columns):
        step = (column + columns - place_ref[1]) % columns
        parts = [jnp.zeros((tokens, LANES), jnp.float32)] * cores
        for group in range(heads // columns):
            block = x_ref[group * columns + column].astype(jnp.float32)
            for core in range(cores):
                home = group * quarter
                top = pltpu.roll(block, (home - core * quarter) % LANES, 1)
                bottom = pltpu.roll(block, (home - core * quarter - HEAD_DIM) % LANES, 1)[:rest]
                moved = jnp.concatenate([top, bottom], axis=0)
                inside = (lane >= home) & (lane < home + quarter)
                parts[core] = jnp.where(inside, moved, parts[core])
        mine_ref[step] = jnp.where(first_core, parts[0], parts[1]).astype(jnp.bfloat16)
        away_ref[step] = jnp.where(first_core, parts[1], parts[0]).astype(jnp.bfloat16)


def weight_open_kernel(x_ref, out_ref):
    for plane in range(x_ref.shape[0]):
        out_ref[:, plane * LANES : (plane + 1) * LANES] = x_ref[plane]


def weight_line_kernel(place_ref, *refs):
    pieces, out_ref = refs[:-1], refs[-1]
    lines = out_ref.shape[0]
    for step, piece_ref in enumerate(pieces):
        out_ref[(place_ref[1] + lines - step) % lines] = piece_ref[...]


def stack_kernel(*refs):
    for step, piece_ref in enumerate(refs[:-1]):
        refs[-1][step] = piece_ref[...]


def dot_tn(a, b):
    return lax.dot_general(a, b, (((0,), (0,)), ((), ())), preferred_element_type=jnp.float32)


def product_kernel(place_ref, own_ref, other_ref, *refs):
    columns = own_ref.shape[0]
    pieces, (block_ref,) = refs[:columns], refs[-1:]
    outs = refs[columns:-1]
    lines, w_cols, model = block_ref.shape
    width = 4 * LANES
    own = jnp.concatenate([piece[0] for piece in pieces], axis=0)
    other = jnp.concatenate([piece[1] for piece in pieces], axis=0)
    rows = own.shape[0]
    for base in range(0, model, width):
        cols = slice(base, base + width)
        total = dot_tn(own, own_ref[:, :, cols].reshape(rows, width))
        total = total + dot_tn(other, other_ref[:, :, cols].reshape(rows, width))
        block_ref[:, :, cols] = total.astype(jnp.bfloat16).reshape(lines, w_cols, width)
    for step, out_ref in enumerate(outs):
        out_ref[...] = block_ref[(place_ref[2] + step) % lines]


def input_grad_kernel(place_ref, both_ref, *refs):
    columns, cores, tokens, _ = both_ref.shape
    weight_ref = refs[-1]
    mine_ref, away_ref = refs[-3:-1]
    lines, w_cols = weight_ref.shape[1:3]
    for step, piece_ref in enumerate(refs[:-3]):
        for column in range(columns):
            weight_ref[column, (place_ref[2] + lines - step) % lines] = piece_ref[
                column * w_cols : (column + 1) * w_cols
            ]
    width = 4 * LANES
    for base in range(0, mine_ref.shape[1], width):
        cols = slice(base, base + width)
        total = jnp.zeros((cores * tokens, width), jnp.float32)
        for step in range(columns):
            weight = weight_ref[(place_ref[1] + step) % columns, :, :, cols]
            total = total + dot_nn(
                both_ref[step].reshape(cores * tokens, LANES), weight.reshape(LANES, width)
            )
        mine_ref[:, cols] = total[:tokens]
        away_ref[:, cols] = total[tokens:].astype(jnp.bfloat16)


def unpack_pair_kernel(x_ref, q_ref, k_ref):
    heads, tokens, _ = x_ref.shape
    low = low_lanes((tokens, LANES))
    for pair in range(heads // 2):
        first = x_ref[2 * pair].astype(jnp.float32)
        second = x_ref[2 * pair + 1].astype(jnp.float32)
        cols = slice(pair * LANES, (pair + 1) * LANES)
        q_ref[:, cols] = jnp.where(low, first, rolled(second)).astype(jnp.bfloat16)
        k_ref[:, cols] = jnp.where(low, rolled(first), second).astype(jnp.bfloat16)


def exchanged(x, axis):
    return lax.all_to_all(x, axis, split_axis=0, concat_axis=0, tiled=True)


def shifted(x, axis, step):
    count = lax.axis_size(axis)
    return lax.ppermute(x, axis, [(place, (place + step) % count) for place in range(count)])


def from_all(x, axis):
    return [x] + [shifted(x, axis, step) for step in range(1, lax.axis_size(axis))]


def near(x):
    return pltpu.with_memory_space_constraint(x, pltpu.VMEM)


def shaped(*shape, dtype=jnp.bfloat16):
    return jax.ShapeDtypeStruct(shape, dtype)


def shards(inputs, query_vectors, key_vectors, value_vectors, cotangent, gate_prefix, value_weight):
    planes = lax.axis_size("sp")
    columns, lines = lax.axis_size("x"), lax.axis_size("y")
    core = lax.axis_index("core")
    tokens, model = inputs.shape[1:]
    width = query_vectors.shape[2]
    heads = width // HEAD_DIM
    length = planes * tokens
    w_cols = value_weight.shape[1]
    weight_block = jnp.broadcast_to(value_weight.T, (planes, w_cols, model // planes))
    weight_block = exchanged(weight_block, "sp")
    place = jnp.stack([core, lax.axis_index("x"), lax.axis_index("y")]).astype(jnp.int32)
    small, whole = pl.BlockSpec(memory_space=pltpu.SMEM), pl.BlockSpec(memory_space=pltpu.VMEM)
    weight_block = pl.pallas_call(weight_open_kernel, out_shape=shaped(w_cols, model))(
        near(weight_block)
    )
    packed = pl.pallas_call(pack_kernel, out_shape=shaped(heads, tokens, 2 * LANES))(
        query_vectors[0], key_vectors[0], value_vectors[0], cotangent[0]
    )
    arrived = exchanged(packed, "sp")
    own_rows = pl.pallas_call(stack_kernel, out_shape=shaped(columns, tokens, model))(
        inputs[0], *map(near, from_all(inputs[0], "x")[1:])
    )
    other_rows = shifted(own_rows, "core", 1)
    weight_line = pl.pallas_call(
        weight_line_kernel,
        out_shape=shaped(columns, w_cols, model),
        in_specs=[small] + [whole] * columns,
    )(place, weight_block, *map(near, from_all(weight_block, "x")[1:]))
    weight_line = weight_line.reshape(columns * w_cols, model)
    weight_pieces = from_all(weight_line, "y")
    kept = (tokens // 2 + 7) // 8 * 8
    sequence = near(arrived.reshape(length, 2 * LANES))
    wide, tile = pltpu.VMEM((length, LANES), jnp.float32), pltpu.VMEM((length, TILE), jnp.float32)
    row = shaped(1, length, dtype=jnp.float32)
    value_grad, peak, share = pl.pallas_call(
        value_kernel,
        out_shape=(shaped(planes, kept, LANES), row, row),
        scratch_shapes=[pltpu.VMEM((length, LANES), jnp.bfloat16), wide, wide, tile],
    )(sequence, gate_prefix[0])
    value_back = exchanged(value_grad, "sp")
    pair_grad = pl.pallas_call(
        pair_kernel,
        out_shape=shaped(length, LANES),
        scratch_shapes=[
            pltpu.VMEM((length, LANES), jnp.bfloat16),
            pltpu.VMEM((HEAD_DIM, length), jnp.bfloat16),
            wide,
            wide,
            tile,
            tile,
        ],
    )(sequence, gate_prefix[0], peak, share)
    pair_back = exchanged(pair_grad.reshape(planes, tokens, LANES), "sp")
    block = shaped(columns, tokens, LANES)
    mine, away = pl.pallas_call(
        unpack_value_kernel, out_shape=(block, block), in_specs=[small, whole]
    )(place, near(value_back))
    both = jnp.stack([mine, shifted(away, "core", 1)], axis=1)
    pieces = [both[0]] + [shifted(both[step], "x", step) for step in range(1, columns)]
    partial = pl.pallas_call(
        product_kernel,
        out_shape=(shaped(w_cols, model),) * lines,
        in_specs=[small] + [whole] * (2 + columns),
        scratch_shapes=[pltpu.VMEM((lines, w_cols, model), jnp.bfloat16)],
    )(place, own_rows, near(other_rows), *map(near, pieces))
    partial = [partial[0]] + [shifted(partial[step], "y", step) for step in range(1, lines)]
    partial = sum(part.astype(jnp.float32) for part in partial).astype(jnp.bfloat16)
    partial = jnp.moveaxis(partial.reshape(w_cols, planes, model // planes), 1, 0)
    partial = exchanged(partial, "sp")
    weight_grad = partial.astype(jnp.float32).sum(axis=0).T
    query_grad, key_grad = pl.pallas_call(
        unpack_pair_kernel, out_shape=(shaped(tokens, width), shaped(tokens, width))
    )(near(pair_back))
    kept_part, sent_part = pl.pallas_call(
        input_grad_kernel,
        out_shape=(shaped(tokens, model, dtype=jnp.float32), shaped(tokens, model)),
        in_specs=[small] + [whole] * (1 + lines),
        scratch_shapes=[pltpu.VMEM((columns, lines, w_cols, model), jnp.bfloat16)],
    )(place, both, *weight_pieces)
    input_grad = (kept_part + shifted(sent_part, "core", 1)).astype(jnp.bfloat16)
    return (query_grad[None], key_grad[None], input_grad[None], weight_grad)


def solution(mesh):
    grid = Mesh(mesh.devices.reshape(-1, 4, 4, 2), ("sp", "y", "x", "core"))
    rows = P(("y", "x", "core"), "sp", None)
    weight = P("sp", ("y", "x", "core"))

    return jax.shard_map(
        shards,
        mesh=grid,
        in_specs=(rows,) * 6 + (weight,),
        out_specs=(rows, rows, rows, weight),
        check_vma=False,
    )
```

```python
import jax
import jax.numpy as jnp
from jax import lax
from jax.experimental import pallas as pl
from jax.experimental.pallas import tpu as pltpu
from jax.sharding import Mesh, PartitionSpec as P

HEAD_DIM = 64
LANES = 128
TILE = 256
FLOOR = -1e30
VMEM_BYTES = 24 * 1024 * 1024


def rolled(x):
    return pltpu.roll(x, HEAD_DIM, 1)


def low_lanes(shape):
    return lax.broadcasted_iota(jnp.int32, shape, 1) < HEAD_DIM


def pack_kernel(q_ref, k_ref, v_ref, g_ref, out_ref):
    heads, tokens, _ = out_ref.shape
    low = low_lanes((tokens, LANES))
    for pair in range(heads // 2):
        cols = slice(pair * LANES, (pair + 1) * LANES)
        for first_ref, second_ref, lane in ((q_ref, k_ref, 0), (v_ref, g_ref, LANES)):
            first = first_ref[:, cols].astype(jnp.float32)
            second = second_ref[:, cols].astype(jnp.float32)
            out_ref[2 * pair, :, lane : lane + LANES] = jnp.where(
                low, first, rolled(second)
            ).astype(jnp.bfloat16)
            out_ref[2 * pair + 1, :, lane : lane + LANES] = jnp.where(
                low, rolled(first), second
            ).astype(jnp.bfloat16)


def dot_nt(a, b):
    return lax.dot_general(a, b, (((1,), (1,)), ((), ())), preferred_element_type=jnp.float32)


def dot_nn(a, b):
    return lax.dot_general(a, b, (((1,), (0,)), ((), ())), preferred_element_type=jnp.float32)


def folded(x, op):
    return op(x.reshape(x.shape[0] // 8, 8, x.shape[1]), axis=0)


def blocks_of(length):
    return [(base, min(TILE, length - base)) for base in range(0, length, TILE)]


def spread(x_ref, p_ref, kq_ref, pc_ref, acc_ref, kt_ref=None):
    for base, rows in blocks_of(x_ref.shape[0]):
        here = slice(base, base + rows)
        swapped = rolled(x_ref[here, :LANES].astype(jnp.float32))
        kq_ref[here] = swapped.astype(jnp.bfloat16)
        if kt_ref is not None:
            kt_ref[:, here] = swapped.T[:HEAD_DIM].astype(jnp.bfloat16)
        pc_ref[here] = jnp.broadcast_to(p_ref[:, here], (LANES, rows)).T
        acc_ref[here] = jnp.zeros((rows, LANES), jnp.float32)


def query_block(x_ref, here, low):
    wide = x_ref[here, :LANES].astype(jnp.float32)
    scaled = jnp.where(low, wide * HEAD_DIM**-0.5, 0.0).astype(jnp.bfloat16)
    return scaled, jnp.where(low, 0.0, rolled(wide)).astype(jnp.bfloat16)


def grad_block(x_ref, here, low):
    wide = rolled(x_ref[here, LANES:].astype(jnp.float32))
    return jnp.where(low, wide, 0.0).astype(jnp.bfloat16)


def score_tile(kq_ref, pc_ref, query_low, q_base, u_base, u_rows):
    q_rows = query_low.shape[0]
    shift = pc_ref[q_base : q_base + 1, :] - pc_ref[u_base : u_base + u_rows]
    shift = jnp.concatenate([shift] * (q_rows // LANES), axis=1)
    scores = dot_nt(kq_ref[u_base : u_base + u_rows], query_low) + shift
    if u_base != q_base:
        return scores
    place = lax.broadcasted_iota(jnp.int32, scores.shape, 0)
    seen = place <= lax.broadcasted_iota(jnp.int32, scores.shape, 1)
    return jnp.where(seen, scores, FLOOR)


def value_kernel(x_ref, p_ref, v_out_ref, peak_ref, share_ref, kq_ref, pc_ref, acc_ref, s_ref):
    length = x_ref.shape[0]
    blocks = blocks_of(length)
    spread(x_ref, p_ref, kq_ref, pc_ref, acc_ref)
    for index, (q_base, q_rows) in enumerate(blocks):
        q_here = slice(q_base, q_base + q_rows)
        low = low_lanes((q_rows, LANES))
        query_low, _ = query_block(x_ref, q_here, low)
        grad_low = grad_block(x_ref, q_here, low)
        peak = jnp.full((8, q_rows), FLOOR, jnp.float32)
        for u_base, u_rows in blocks[: index + 1]:
            scores = score_tile(kq_ref, pc_ref, query_low, q_base, u_base, u_rows)
            s_ref[u_base : u_base + u_rows, :q_rows] = scores
            peak = jnp.maximum(peak, folded(scores, jnp.max))
        peak = jnp.max(peak, axis=0, keepdims=True)
        total = jnp.zeros((8, q_rows), jnp.float32)
        for u_base, u_rows in blocks[: index + 1]:
            u_here = slice(u_base, u_base + u_rows)
            raised = jnp.exp(s_ref[u_here, :q_rows] - peak)
            s_ref[u_here, :q_rows] = raised
            total = total + folded(raised, jnp.sum)
        share = 1.0 / jnp.sum(total, axis=0, keepdims=True)
        peak_ref[:, q_here] = peak
        share_ref[:, q_here] = share
        for u_base, u_rows in blocks[: index + 1]:
            u_here = slice(u_base, u_base + u_rows)
            soft = s_ref[u_here, :q_rows] * share
            acc_ref[u_here] += dot_nn(soft.astype(jnp.bfloat16), grad_low)
    planes, kept, _ = v_out_ref.shape
    tokens = length // planes
    for plane in range(planes):
        base = plane * tokens
        first = acc_ref[base : base + kept]
        second = acc_ref[base + kept : base + tokens]
        second = jnp.concatenate([second, first[: 2 * kept - tokens]], axis=0)
        v_out_ref[plane] = jnp.where(low_lanes(first.shape), first, rolled(second)).astype(
            jnp.bfloat16
        )


def pair_kernel(
    x_ref, p_ref, peak_ref, share_ref, qk_ref, kq_ref, kt_ref, pc_ref, acc_ref, s_ref, d_ref
):
    blocks = blocks_of(x_ref.shape[0])
    scale = HEAD_DIM**-0.5
    spread(x_ref, p_ref, kq_ref, pc_ref, acc_ref, kt_ref)
    for index, (q_base, q_rows) in enumerate(blocks):
        q_here = slice(q_base, q_base + q_rows)
        low = low_lanes((q_rows, LANES))
        query_low, query_high = query_block(x_ref, q_here, low)
        grad_low = grad_block(x_ref, q_here, low)
        peak = peak_ref[:, q_here]
        share = share_ref[:, q_here]
        term = jnp.zeros((8, q_rows), jnp.float32)
        for u_base, u_rows in blocks[: index + 1]:
            u_here = slice(u_base, u_base + u_rows)
            scores = score_tile(kq_ref, pc_ref, query_low, q_base, u_base, u_rows)
            soft = jnp.exp(scores - peak) * share
            s_ref[u_here, :q_rows] = soft
            soft_grad = dot_nt(x_ref[u_here, LANES:], grad_low)
            d_ref[u_here, :q_rows] = soft_grad
            term = term + folded(soft * soft_grad, jnp.sum)
        term = jnp.sum(term, axis=0, keepdims=True)
        query_grad = jnp.zeros((HEAD_DIM, q_rows), jnp.float32)
        for u_base, u_rows in blocks[: index + 1]:
            u_here = slice(u_base, u_base + u_rows)
            score_low = (s_ref[u_here, :q_rows] * (d_ref[u_here, :q_rows] - term)).astype(
                jnp.bfloat16
            )
            acc_ref[u_here] += dot_nn(score_low, query_high)
            query_grad = query_grad + dot_nn(kt_ref[:, u_here], score_low)
        query_grad = jnp.concatenate([query_grad, jnp.zeros_like(query_grad)], axis=0)
        acc_ref[q_here] += query_grad.T
    for base, rows in blocks:
        here = slice(base, base + rows)
        qk_ref[here] = (acc_ref[here] * scale).astype(jnp.bfloat16)


def unpack_value_kernel(place_ref, x_ref, mine_ref, away_ref):
    heads, kept, _ = x_ref.shape
    columns, tokens, _ = mine_ref.shape
    rest = tokens - kept
    cores = HEAD_DIM * columns // LANES
    quarter = HEAD_DIM // cores
    lane = lax.broadcasted_iota(jnp.int32, (tokens, LANES), 1)
    first_core = place_ref[0] == 0
    for column in range(columns):
        step = (column + columns - place_ref[1]) % columns
        parts = [jnp.zeros((tokens, LANES), jnp.float32)] * cores
        for group in range(heads // columns):
            block = x_ref[group * columns + column].astype(jnp.float32)
            for core in range(cores):
                home = group * quarter
                top = pltpu.roll(block, (home - core * quarter) % LANES, 1)
                bottom = pltpu.roll(block, (home - core * quarter - HEAD_DIM) % LANES, 1)[:rest]
                moved = jnp.concatenate([top, bottom], axis=0)
                inside = (lane >= home) & (lane < home + quarter)
                parts[core] = jnp.where(inside, moved, parts[core])
        mine_ref[step] = jnp.where(first_core, parts[0], parts[1]).astype(jnp.bfloat16)
        away_ref[step] = jnp.where(first_core, parts[1], parts[0]).astype(jnp.bfloat16)


def weight_open_kernel(x_ref, out_ref):
    for plane in range(x_ref.shape[0]):
        out_ref[:, plane * LANES : (plane + 1) * LANES] = x_ref[plane]


def weight_line_kernel(place_ref, *refs):
    pieces, out_ref = refs[:-1], refs[-1]
    lines = out_ref.shape[0]
    for step, piece_ref in enumerate(pieces):
        out_ref[(place_ref[1] + lines - step) % lines] = piece_ref[...]


def stack_kernel(*refs):
    for step, piece_ref in enumerate(refs[:-1]):
        refs[-1][step] = piece_ref[...]


def dot_tn(a, b):
    return lax.dot_general(a, b, (((0,), (0,)), ((), ())), preferred_element_type=jnp.float32)


def product_kernel(place_ref, own_ref, other_ref, *refs):
    columns = own_ref.shape[0]
    pieces, (block_ref,) = refs[:columns], refs[-1:]
    outs = refs[columns:-1]
    lines, w_cols, model = block_ref.shape
    width = 4 * LANES
    own = jnp.concatenate([piece[0] for piece in pieces], axis=0)
    other = jnp.concatenate([piece[1] for piece in pieces], axis=0)
    rows = own.shape[0]
    for base in range(0, model, width):
        cols = slice(base, base + width)
        total = dot_tn(own, own_ref[:, :, cols].reshape(rows, width))
        total = total + dot_tn(other, other_ref[:, :, cols].reshape(rows, width))
        block_ref[:, :, cols] = total.astype(jnp.bfloat16).reshape(lines, w_cols, width)
    for step, out_ref in enumerate(outs):
        out_ref[...] = block_ref[(place_ref[2] + step) % lines]


def input_grad_kernel(place_ref, first_ref, second_ref, *refs):
    columns, tokens, _ = first_ref.shape
    weight_ref = refs[-1]
    mine_ref, away_ref = refs[-3:-1]
    lines, w_cols = weight_ref.shape[1:3]
    for step, piece_ref in enumerate(refs[:-3]):
        for column in range(columns):
            weight_ref[column, (place_ref[2] + lines - step) % lines] = piece_ref[
                column * w_cols : (column + 1) * w_cols
            ]
    width = 4 * LANES
    for base in range(0, mine_ref.shape[1], width):
        cols = slice(base, base + width)
        first = jnp.zeros((tokens, width), jnp.float32)
        second = jnp.zeros((tokens, width), jnp.float32)
        for step in range(columns):
            weight = weight_ref[(place_ref[1] + step) % columns, :, :, cols]
            weight = weight.reshape(LANES, width)
            first = first + dot_nn(first_ref[step], weight)
            second = second + dot_nn(second_ref[step], weight)
        mine_ref[:, cols] = first
        away_ref[:, cols] = second.astype(jnp.bfloat16)


def add_kernel(first_ref, second_ref, out_ref):
    total = first_ref[...] + second_ref[...].astype(jnp.float32)
    out_ref[...] = total.astype(jnp.bfloat16)


def unpack_pair_kernel(x_ref, q_ref, k_ref):
    heads, tokens, _ = x_ref.shape
    low = low_lanes((tokens, LANES))
    for pair in range(heads // 2):
        first = x_ref[2 * pair].astype(jnp.float32)
        second = x_ref[2 * pair + 1].astype(jnp.float32)
        cols = slice(pair * LANES, (pair + 1) * LANES)
        q_ref[:, cols] = jnp.where(low, first, rolled(second)).astype(jnp.bfloat16)
        k_ref[:, cols] = jnp.where(low, rolled(first), second).astype(jnp.bfloat16)


def exchanged(x, axis):
    return lax.all_to_all(x, axis, split_axis=0, concat_axis=0, tiled=True)


def shifted(x, axis, step):
    count = lax.axis_size(axis)
    return lax.ppermute(x, axis, [(place, (place + step) % count) for place in range(count)])


def from_all(x, axis):
    return [x] + [shifted(x, axis, step) for step in range(1, lax.axis_size(axis))]


def near(x):
    return pltpu.with_memory_space_constraint(x, pltpu.VMEM)


def shaped(*shape, dtype=jnp.bfloat16):
    return jax.ShapeDtypeStruct(shape, dtype)


def shards(inputs, query_vectors, key_vectors, value_vectors, cotangent, gate_prefix, value_weight):
    planes = lax.axis_size("sp")
    columns, lines = lax.axis_size("x"), lax.axis_size("y")
    core = lax.axis_index("core")
    tokens, model = inputs.shape[1:]
    width = query_vectors.shape[2]
    heads = width // HEAD_DIM
    length = planes * tokens
    w_cols = value_weight.shape[1]
    weight_block = jnp.broadcast_to(value_weight.T, (planes, w_cols, model // planes))
    weight_block = exchanged(weight_block, "sp")
    place = jnp.stack([core, lax.axis_index("x"), lax.axis_index("y")]).astype(jnp.int32)
    small, whole = pl.BlockSpec(memory_space=pltpu.SMEM), pl.BlockSpec(memory_space=pltpu.VMEM)
    weight_block = pl.pallas_call(weight_open_kernel, out_shape=shaped(w_cols, model))(
        near(weight_block)
    )
    packed = pl.pallas_call(pack_kernel, out_shape=shaped(heads, tokens, 2 * LANES))(
        query_vectors[0], key_vectors[0], value_vectors[0], cotangent[0]
    )
    arrived = exchanged(packed, "sp")
    own_rows = pl.pallas_call(stack_kernel, out_shape=shaped(columns, tokens, model))(
        inputs[0], *map(near, from_all(inputs[0], "x")[1:])
    )
    other_rows = shifted(own_rows, "core", 1)
    weight_line = pl.pallas_call(
        weight_line_kernel,
        out_shape=shaped(columns, w_cols, model),
        in_specs=[small] + [whole] * columns,
    )(place, weight_block, *map(near, from_all(weight_block, "x")[1:]))
    weight_line = weight_line.reshape(columns * w_cols, model)
    weight_pieces = from_all(weight_line, "y")
    kept = (tokens // 2 + 7) // 8 * 8
    sequence = near(arrived.reshape(length, 2 * LANES))
    wide, tile = pltpu.VMEM((length, LANES), jnp.float32), pltpu.VMEM((length, TILE), jnp.float32)
    row = shaped(1, length, dtype=jnp.float32)
    value_grad, peak, share = pl.pallas_call(
        value_kernel,
        out_shape=(shaped(planes, kept, LANES), row, row),
        scratch_shapes=[pltpu.VMEM((length, LANES), jnp.bfloat16), wide, wide, tile],
    )(sequence, gate_prefix[0])
    value_back = exchanged(value_grad, "sp")
    pair_grad = pl.pallas_call(
        pair_kernel,
        out_shape=shaped(length, LANES),
        scratch_shapes=[
            pltpu.VMEM((length, LANES), jnp.bfloat16),
            pltpu.VMEM((HEAD_DIM, length), jnp.bfloat16),
            wide,
            wide,
            tile,
            tile,
        ],
    )(sequence, gate_prefix[0], peak, share)
    pair_back = exchanged(pair_grad.reshape(planes, tokens, LANES), "sp")
    block = shaped(columns, tokens, LANES)
    mine, away = pl.pallas_call(
        unpack_value_kernel, out_shape=(block, block), in_specs=[small, whole]
    )(place, near(value_back))
    brought = shifted(away, "core", 1)
    both = jnp.stack([mine, brought], axis=1)
    pieces = [both[0]] + [shifted(both[step], "x", step) for step in range(1, columns)]
    partial = pl.pallas_call(
        product_kernel,
        compiler_params=pltpu.CompilerParams(vmem_limit_bytes=VMEM_BYTES),
        out_shape=(shaped(w_cols, model),) * lines,
        in_specs=[small] + [whole] * (2 + columns),
        scratch_shapes=[pltpu.VMEM((lines, w_cols, model), jnp.bfloat16)],
    )(place, near(own_rows), near(other_rows), *map(near, pieces))
    partial = [partial[0]] + [shifted(partial[step], "y", step) for step in range(1, lines)]
    partial = sum(part.astype(jnp.float32) for part in partial).astype(jnp.bfloat16)
    partial = jnp.moveaxis(partial.reshape(w_cols, planes, model // planes), 1, 0)
    partial = exchanged(partial, "sp")
    weight_grad = partial.astype(jnp.float32).sum(axis=0).T
    query_grad, key_grad = pl.pallas_call(
        unpack_pair_kernel, out_shape=(shaped(tokens, width), shaped(tokens, width))
    )(near(pair_back))
    kept_part, sent_part = pl.pallas_call(
        input_grad_kernel,
        out_shape=(shaped(tokens, model, dtype=jnp.float32), shaped(tokens, model)),
        in_specs=[small] + [whole] * (2 + lines),
        scratch_shapes=[pltpu.VMEM((columns, lines, w_cols, model), jnp.bfloat16)],
    )(place, mine, near(brought), *weight_pieces)
    input_grad = pl.pallas_call(add_kernel, out_shape=shaped(tokens, model))(
        kept_part, near(shifted(sent_part, "core", 1))
    )
    return (query_grad[None], key_grad[None], input_grad[None], weight_grad)


def solution(mesh):
    grid = Mesh(mesh.devices.reshape(-1, 4, 4, 2), ("sp", "y", "x", "core"))
    rows = P(("y", "x", "core"), "sp", None)
    weight = P("sp", ("y", "x", "core"))

    return jax.shard_map(
        shards,
        mesh=grid,
        in_specs=(rows,) * 6 + (weight,),
        out_specs=(rows, rows, rows, weight),
        check_vma=False,
    )
```

```python
import jax
import jax.numpy as jnp
from jax import lax
from jax.experimental import pallas as pl
from jax.experimental.pallas import tpu as pltpu
from jax.sharding import Mesh, PartitionSpec as P

HEAD_DIM = 64
LANES = 128
TILE = 256
FLOOR = -1e30
VMEM_BYTES = 24 * 1024 * 1024


def rolled(x):
    return pltpu.roll(x, HEAD_DIM, 1)


def low_lanes(shape):
    return lax.broadcasted_iota(jnp.int32, shape, 1) < HEAD_DIM


def pack_kernel(q_ref, k_ref, v_ref, g_ref, out_ref):
    heads, tokens, _ = out_ref.shape
    low = low_lanes((tokens, LANES))
    for pair in range(heads // 2):
        cols = slice(pair * LANES, (pair + 1) * LANES)
        for first_ref, second_ref, lane in ((q_ref, k_ref, 0), (v_ref, g_ref, LANES)):
            first = first_ref[:, cols].astype(jnp.float32)
            second = second_ref[:, cols].astype(jnp.float32)
            out_ref[2 * pair, :, lane : lane + LANES] = jnp.where(
                low, first, rolled(second)
            ).astype(jnp.bfloat16)
            out_ref[2 * pair + 1, :, lane : lane + LANES] = jnp.where(
                low, rolled(first), second
            ).astype(jnp.bfloat16)


def dot_nt(a, b):
    return lax.dot_general(a, b, (((1,), (1,)), ((), ())), preferred_element_type=jnp.float32)


def dot_nn(a, b):
    return lax.dot_general(a, b, (((1,), (0,)), ((), ())), preferred_element_type=jnp.float32)


def folded(x, op):
    return op(x.reshape(x.shape[0] // 8, 8, x.shape[1]), axis=0)


def blocks_of(length):
    return [(base, min(TILE, length - base)) for base in range(0, length, TILE)]


def spread(x_ref, p_ref, kq_ref, pc_ref, acc_ref, kt_ref=None):
    for base, rows in blocks_of(x_ref.shape[0]):
        here = slice(base, base + rows)
        swapped = rolled(x_ref[here, :LANES].astype(jnp.float32))
        kq_ref[here] = swapped.astype(jnp.bfloat16)
        if kt_ref is not None:
            kt_ref[:, here] = swapped.T[:HEAD_DIM].astype(jnp.bfloat16)
        pc_ref[here] = jnp.broadcast_to(p_ref[:, here], (LANES, rows)).T
        acc_ref[here] = jnp.zeros((rows, LANES), jnp.float32)


def query_block(x_ref, here, low):
    wide = x_ref[here, :LANES].astype(jnp.float32)
    scaled = jnp.where(low, wide * HEAD_DIM**-0.5, 0.0).astype(jnp.bfloat16)
    return scaled, jnp.where(low, 0.0, rolled(wide)).astype(jnp.bfloat16)


def grad_block(x_ref, here, low):
    wide = rolled(x_ref[here, LANES:].astype(jnp.float32))
    return jnp.where(low, wide, 0.0).astype(jnp.bfloat16)


def score_tile(kq_ref, pc_ref, query_low, q_base, u_base, u_rows):
    q_rows = query_low.shape[0]
    shift = pc_ref[q_base : q_base + 1, :] - pc_ref[u_base : u_base + u_rows]
    shift = jnp.concatenate([shift] * (q_rows // LANES), axis=1)
    scores = dot_nt(kq_ref[u_base : u_base + u_rows], query_low) + shift
    if u_base != q_base:
        return scores
    place = lax.broadcasted_iota(jnp.int32, scores.shape, 0)
    seen = place <= lax.broadcasted_iota(jnp.int32, scores.shape, 1)
    return jnp.where(seen, scores, FLOOR)


def value_kernel(x_ref, p_ref, v_out_ref, peak_ref, share_ref, kq_ref, pc_ref, acc_ref, s_ref):
    length = x_ref.shape[0]
    blocks = blocks_of(length)
    spread(x_ref, p_ref, kq_ref, pc_ref, acc_ref)
    for index, (q_base, q_rows) in enumerate(blocks):
        q_here = slice(q_base, q_base + q_rows)
        low = low_lanes((q_rows, LANES))
        query_low, _ = query_block(x_ref, q_here, low)
        grad_low = grad_block(x_ref, q_here, low)
        peak = jnp.full((8, q_rows), FLOOR, jnp.float32)
        for u_base, u_rows in blocks[: index + 1]:
            scores = score_tile(kq_ref, pc_ref, query_low, q_base, u_base, u_rows)
            s_ref[u_base : u_base + u_rows, :q_rows] = scores
            peak = jnp.maximum(peak, folded(scores, jnp.max))
        peak = jnp.max(peak, axis=0, keepdims=True)
        total = jnp.zeros((8, q_rows), jnp.float32)
        for u_base, u_rows in blocks[: index + 1]:
            u_here = slice(u_base, u_base + u_rows)
            raised = jnp.exp(s_ref[u_here, :q_rows] - peak)
            s_ref[u_here, :q_rows] = raised
            total = total + folded(raised, jnp.sum)
        share = 1.0 / jnp.sum(total, axis=0, keepdims=True)
        peak_ref[:, q_here] = peak
        share_ref[:, q_here] = share
        for u_base, u_rows in blocks[: index + 1]:
            u_here = slice(u_base, u_base + u_rows)
            soft = s_ref[u_here, :q_rows] * share
            acc_ref[u_here] += dot_nn(soft.astype(jnp.bfloat16), grad_low)
    planes, cores, kept, _ = v_out_ref.shape
    tokens = length // planes
    quarter = HEAD_DIM // cores
    lane = lax.broadcasted_iota(jnp.int32, (kept, LANES), 1)
    for plane in range(planes):
        for core in range(cores):
            packed = jnp.zeros((kept, LANES), jnp.float32)
            for group in range(LANES // quarter):
                base = plane * tokens + group * kept
                rows = min(kept, tokens - group * kept)
                part = acc_ref[base : base + rows]
                if rows < kept:
                    part = jnp.concatenate([part, jnp.zeros((kept - rows, LANES), jnp.float32)])
                home = group * quarter
                part = pltpu.roll(part, (home - core * quarter) % LANES, 1)
                packed = jnp.where((lane >= home) & (lane < home + quarter), part, packed)
            v_out_ref[plane, core] = packed.astype(jnp.bfloat16)


def pair_kernel(
    x_ref, p_ref, peak_ref, share_ref, qk_ref, kq_ref, kt_ref, pc_ref, acc_ref, s_ref, d_ref
):
    blocks = blocks_of(x_ref.shape[0])
    scale = HEAD_DIM**-0.5
    spread(x_ref, p_ref, kq_ref, pc_ref, acc_ref, kt_ref)
    for index, (q_base, q_rows) in enumerate(blocks):
        q_here = slice(q_base, q_base + q_rows)
        low = low_lanes((q_rows, LANES))
        query_low, query_high = query_block(x_ref, q_here, low)
        grad_low = grad_block(x_ref, q_here, low)
        peak = peak_ref[:, q_here]
        share = share_ref[:, q_here]
        term = jnp.zeros((8, q_rows), jnp.float32)
        for u_base, u_rows in blocks[: index + 1]:
            u_here = slice(u_base, u_base + u_rows)
            scores = score_tile(kq_ref, pc_ref, query_low, q_base, u_base, u_rows)
            soft = jnp.exp(scores - peak) * share
            s_ref[u_here, :q_rows] = soft
            soft_grad = dot_nt(x_ref[u_here, LANES:], grad_low)
            d_ref[u_here, :q_rows] = soft_grad
            term = term + folded(soft * soft_grad, jnp.sum)
        term = jnp.sum(term, axis=0, keepdims=True)
        query_grad = jnp.zeros((HEAD_DIM, q_rows), jnp.float32)
        for u_base, u_rows in blocks[: index + 1]:
            u_here = slice(u_base, u_base + u_rows)
            score_low = (s_ref[u_here, :q_rows] * (d_ref[u_here, :q_rows] - term)).astype(
                jnp.bfloat16
            )
            acc_ref[u_here] += dot_nn(score_low, query_high)
            query_grad = query_grad + dot_nn(kt_ref[:, u_here], score_low)
        query_grad = jnp.concatenate([query_grad, jnp.zeros_like(query_grad)], axis=0)
        acc_ref[q_here] += query_grad.T
    for base, rows in blocks:
        here = slice(base, base + rows)
        qk_ref[here] = (acc_ref[here] * scale).astype(jnp.bfloat16)


def pair_steps(here):
    return [here, 3 - here, here + 1 - 2 * (here % 2), (here + 2) % 4]


def unpack_value_kernel(place_ref, x_ref, own_ref, flip_ref, far_ref):
    cores, tokens, _ = own_ref.shape
    out_refs = [own_ref, flip_ref, far_ref.at[0], far_ref.at[1]]
    columns = len(out_refs)
    heads, kept = x_ref.shape[0] // cores, x_ref.shape[1]
    quarter = HEAD_DIM // cores
    groups = LANES // quarter
    lane = lax.broadcasted_iota(jnp.int32, (tokens, LANES), 1)
    for out_ref, column in zip(out_refs, pair_steps(place_ref[1])):
        for source in range(cores):
            whole = jnp.zeros((tokens, LANES), jnp.float32)
            for line in range(heads // columns):
                block = x_ref[(line * columns + column) * cores + source].astype(jnp.float32)
                home = line * quarter
                rows = [
                    pltpu.roll(block, (home - group * quarter) % LANES, 1)[
                        : min(kept, tokens - group * kept)
                    ]
                    for group in range(groups)
                ]
                moved = jnp.concatenate(rows, axis=0)
                whole = jnp.where((lane >= home) & (lane < home + quarter), moved, whole)
            out_ref[(source + cores - place_ref[0]) % cores] = whole.astype(jnp.bfloat16)


def weight_open_kernel(x_ref, out_ref):
    for plane in range(x_ref.shape[0]):
        out_ref[:, plane * LANES : (plane + 1) * LANES] = x_ref[plane]


def weight_line_kernel(place_ref, *refs):
    pieces, out_ref = refs[:-1], refs[-1]
    lines = out_ref.shape[0]
    for step, piece_ref in enumerate(pieces):
        out_ref[(place_ref[1] + lines - step) % lines] = piece_ref[...]


def stack_kernel(*refs):
    for step, piece_ref in enumerate(refs[:-1]):
        refs[-1][step] = piece_ref[...]


def dot_tn(a, b):
    return lax.dot_general(a, b, (((0,), (0,)), ((), ())), preferred_element_type=jnp.float32)


def product_kernel(place_ref, own_ref, other_ref, here_ref, first_ref, second_ref, *refs):
    outs, block_ref = refs[:-1], refs[-1]
    lines, w_cols, model = block_ref.shape
    width = 4 * LANES
    own, other = (
        jnp.concatenate(
            [here_ref[core], second_ref[0, core], first_ref[0, core], second_ref[1, core]], axis=0
        )
        for core in range(here_ref.shape[0])
    )
    rows = own.shape[0]
    for base in range(0, model, width):
        cols = slice(base, base + width)
        total = dot_tn(own, own_ref[:, :, cols].reshape(rows, width))
        total = total + dot_tn(other, other_ref[:, :, cols].reshape(rows, width))
        block_ref[:, :, cols] = total.astype(jnp.bfloat16).reshape(lines, w_cols, width)
    for step, out_ref in enumerate(outs):
        out_ref[...] = block_ref[(place_ref[2] + step) % lines]


def input_grad_kernel(place_ref, *refs):
    weight_ref = refs[-1]
    columns, lines = weight_ref.shape[:2]
    own_ref, flip_ref, far_ref = refs[:3]
    blocks, refs = [own_ref, flip_ref, far_ref.at[0], far_ref.at[1]], refs[3:]
    tokens = own_ref.shape[1]
    mine_ref, away_ref = refs[-3:-1]
    w_cols = weight_ref.shape[2]
    for step, piece_ref in enumerate(refs[:-3]):
        for column in range(columns):
            weight_ref[column, (place_ref[2] + lines - step) % lines] = piece_ref[
                column * w_cols : (column + 1) * w_cols
            ]
    width = 4 * LANES
    for base in range(0, mine_ref.shape[1], width):
        cols = slice(base, base + width)
        first = jnp.zeros((tokens, width), jnp.float32)
        second = jnp.zeros((tokens, width), jnp.float32)
        for block, column in zip(blocks, pair_steps(place_ref[1])):
            weight = weight_ref[column, :, :, cols].reshape(LANES, width)
            first = first + dot_nn(block[0], weight)
            second = second + dot_nn(block[1], weight)
        mine_ref[:, cols] = first
        away_ref[:, cols] = second.astype(jnp.bfloat16)


def add_kernel(first_ref, second_ref, out_ref):
    total = first_ref[...] + second_ref[...].astype(jnp.float32)
    out_ref[...] = total.astype(jnp.bfloat16)


def unpack_pair_kernel(x_ref, q_ref, k_ref):
    heads, tokens, _ = x_ref.shape
    low = low_lanes((tokens, LANES))
    for pair in range(heads // 2):
        first = x_ref[2 * pair].astype(jnp.float32)
        second = x_ref[2 * pair + 1].astype(jnp.float32)
        cols = slice(pair * LANES, (pair + 1) * LANES)
        q_ref[:, cols] = jnp.where(low, first, rolled(second)).astype(jnp.bfloat16)
        k_ref[:, cols] = jnp.where(low, rolled(first), second).astype(jnp.bfloat16)


def exchanged(x, axis):
    return lax.all_to_all(x, axis, split_axis=0, concat_axis=0, tiled=True)


def shifted(x, axis, step):
    count = lax.axis_size(axis)
    return lax.ppermute(x, axis, [(place, (place + step) % count) for place in range(count)])


def paired(x, step):
    return lax.ppermute(x, "x", [(place, pair_steps(place)[step]) for place in range(4)])


def from_all(x, axis):
    return [x] + [shifted(x, axis, step) for step in range(1, lax.axis_size(axis))]


def near(x):
    return pltpu.with_memory_space_constraint(x, pltpu.VMEM)


def shaped(*shape, dtype=jnp.bfloat16):
    return jax.ShapeDtypeStruct(shape, dtype)


def shards(inputs, query_vectors, key_vectors, value_vectors, cotangent, gate_prefix, value_weight):
    planes = lax.axis_size("sp")
    cores, columns, lines = lax.axis_size("core"), lax.axis_size("x"), lax.axis_size("y")
    core = lax.axis_index("core")
    tokens, model = inputs.shape[1:]
    width = query_vectors.shape[2]
    heads = width // HEAD_DIM
    length = planes * tokens
    w_cols = value_weight.shape[1]
    weight_block = jnp.broadcast_to(value_weight.T, (planes, w_cols, model // planes))
    weight_block = exchanged(weight_block, "sp")
    place = jnp.stack([core, lax.axis_index("x"), lax.axis_index("y")]).astype(jnp.int32)
    small, whole = pl.BlockSpec(memory_space=pltpu.SMEM), pl.BlockSpec(memory_space=pltpu.VMEM)
    weight_block = pl.pallas_call(weight_open_kernel, out_shape=shaped(w_cols, model))(
        near(weight_block)
    )
    packed = pl.pallas_call(pack_kernel, out_shape=shaped(heads, tokens, 2 * LANES))(
        query_vectors[0], key_vectors[0], value_vectors[0], cotangent[0]
    )
    arrived = exchanged(packed, "sp")
    own_rows = pl.pallas_call(stack_kernel, out_shape=shaped(columns, tokens, model))(
        inputs[0], *[near(paired(inputs[0], step)) for step in range(1, columns)]
    )
    other_rows = shifted(own_rows, "core", 1)
    weight_line = pl.pallas_call(
        weight_line_kernel,
        out_shape=shaped(columns, w_cols, model),
        in_specs=[small] + [whole] * columns,
    )(place, weight_block, *map(near, from_all(weight_block, "x")[1:]))
    weight_line = weight_line.reshape(columns * w_cols, model)
    weight_pieces = from_all(weight_line, "y")
    kept = (tokens // (2 * cores) + 7) // 8 * 8
    sequence = near(arrived.reshape(length, 2 * LANES))
    wide, tile = pltpu.VMEM((length, LANES), jnp.float32), pltpu.VMEM((length, TILE), jnp.float32)
    row = shaped(1, length, dtype=jnp.float32)
    value_grad, peak, share = pl.pallas_call(
        value_kernel,
        out_shape=(shaped(planes, cores, kept, LANES), row, row),
        scratch_shapes=[pltpu.VMEM((length, LANES), jnp.bfloat16), wide, wide, tile],
    )(sequence, gate_prefix[0])
    value_back = exchanged(value_grad.reshape(planes * cores, kept, LANES), ("sp", "core"))
    pair_grad = pl.pallas_call(
        pair_kernel,
        out_shape=shaped(length, LANES),
        scratch_shapes=[
            pltpu.VMEM((length, LANES), jnp.bfloat16),
            pltpu.VMEM((HEAD_DIM, length), jnp.bfloat16),
            wide,
            wide,
            tile,
            tile,
        ],
    )(sequence, gate_prefix[0], peak, share)
    pair_back = exchanged(pair_grad.reshape(planes, tokens, LANES), "sp")
    block = shaped(cores, tokens, LANES)
    blocks = pl.pallas_call(
        unpack_value_kernel,
        out_shape=(block, block, shaped(2, cores, tokens, LANES)),
        in_specs=[small, whole],
    )(place, near(value_back))
    first = paired(blocks[2], 2)
    second = paired(jnp.stack([blocks[1], first[1]]), 1)
    partial = pl.pallas_call(
        product_kernel,
        compiler_params=pltpu.CompilerParams(vmem_limit_bytes=VMEM_BYTES),
        out_shape=(shaped(w_cols, model),) * lines,
        in_specs=[small] + [whole] * 5,
        scratch_shapes=[pltpu.VMEM((lines, w_cols, model), jnp.bfloat16)],
    )(place, near(own_rows), near(other_rows), blocks[0], near(first), near(second))
    partial = [partial[0]] + [shifted(partial[step], "y", step) for step in range(1, lines)]
    partial = sum(part.astype(jnp.float32) for part in partial).astype(jnp.bfloat16)
    partial = jnp.moveaxis(partial.reshape(w_cols, planes, model // planes), 1, 0)
    partial = exchanged(partial, "sp")
    weight_grad = partial.astype(jnp.float32).sum(axis=0).T
    query_grad, key_grad = pl.pallas_call(
        unpack_pair_kernel, out_shape=(shaped(tokens, width), shaped(tokens, width))
    )(near(pair_back))
    kept_part, sent_part = pl.pallas_call(
        input_grad_kernel,
        out_shape=(shaped(tokens, model, dtype=jnp.float32), shaped(tokens, model)),
        in_specs=[small] + [whole] * (3 + lines),
        scratch_shapes=[pltpu.VMEM((columns, lines, w_cols, model), jnp.bfloat16)],
    )(place, *blocks, *weight_pieces)
    input_grad = pl.pallas_call(add_kernel, out_shape=shaped(tokens, model))(
        kept_part, near(shifted(sent_part, "core", 1))
    )
    return (query_grad[None], key_grad[None], input_grad[None], weight_grad)


def solution(mesh):
    grid = Mesh(mesh.devices.reshape(-1, 4, 4, 2), ("sp", "y", "x", "core"))
    rows = P(("y", "x", "core"), "sp", None)
    weight = P("sp", ("y", "x", "core"))

    return jax.shard_map(
        shards,
        mesh=grid,
        in_specs=(rows,) * 6 + (weight,),
        out_specs=(rows, rows, rows, weight),
        check_vma=False,
    )
```

```python
import jax
import jax.numpy as jnp
from jax import lax
from jax.experimental import pallas as pl
from jax.experimental.pallas import tpu as pltpu
from jax.sharding import Mesh, PartitionSpec as P

HEAD_DIM = 64
LANES = 128
TILE = 256
FLOOR = -1e30
VMEM_BYTES = 24 * 1024 * 1024


def rolled(x):
    return pltpu.roll(x, HEAD_DIM, 1)


def low_lanes(shape):
    return lax.broadcasted_iota(jnp.int32, shape, 1) < HEAD_DIM


def pack_kernel(q_ref, k_ref, v_ref, g_ref, w_ref, first_ref, second_ref):
    heads, tokens, _ = second_ref.shape
    low = low_lanes((tokens, LANES))
    for pair in range(heads // 2):
        cols = slice(pair * LANES, (pair + 1) * LANES)
        for one_ref, two_ref, out_ref in ((q_ref, k_ref, first_ref), (v_ref, g_ref, second_ref)):
            one = one_ref[:, cols].astype(jnp.float32)
            two = two_ref[:, cols].astype(jnp.float32)
            out_ref[2 * pair, :tokens] = jnp.where(low, one, rolled(two)).astype(jnp.bfloat16)
            out_ref[2 * pair + 1, :tokens] = jnp.where(low, rolled(one), two).astype(jnp.bfloat16)
    for head in range(heads):
        first_ref[head, tokens:] = w_ref[...]


def open_kernel(x_ref, qk_ref, weight_ref):
    planes, tokens, _ = qk_ref.shape
    for plane in range(planes):
        qk_ref[plane] = x_ref[plane, :tokens]
        weight_ref[:, plane * LANES : (plane + 1) * LANES] = x_ref[plane, tokens:]


def dot_nt(a, b):
    return lax.dot_general(a, b, (((1,), (1,)), ((), ())), preferred_element_type=jnp.float32)


def dot_nn(a, b):
    return lax.dot_general(a, b, (((1,), (0,)), ((), ())), preferred_element_type=jnp.float32)


def folded(x, op):
    return op(x.reshape(x.shape[0] // 8, 8, x.shape[1]), axis=0)


def blocks_of(length):
    return [(base, min(TILE, length - base)) for base in range(0, length, TILE)]


def spread(x_ref, p_ref, kq_ref, pc_ref, acc_ref=None, kt_ref=None):
    for base, rows in blocks_of(x_ref.shape[0]):
        here = slice(base, base + rows)
        swapped = rolled(x_ref[here].astype(jnp.float32))
        kq_ref[here] = swapped.astype(jnp.bfloat16)
        if kt_ref is not None:
            kt_ref[:, here] = swapped.T[:HEAD_DIM].astype(jnp.bfloat16)
        pc_ref[here] = jnp.broadcast_to(p_ref[:, here], (LANES, rows)).T
        if acc_ref is not None:
            acc_ref[here] = jnp.zeros((rows, LANES), jnp.float32)


def query_block(x_ref, here, low):
    wide = x_ref[here].astype(jnp.float32)
    scaled = jnp.where(low, wide * HEAD_DIM**-0.5, 0.0).astype(jnp.bfloat16)
    return scaled, jnp.where(low, 0.0, rolled(wide)).astype(jnp.bfloat16)


def grad_block(x_ref, here, low):
    wide = rolled(x_ref[here].astype(jnp.float32))
    return jnp.where(low, wide, 0.0).astype(jnp.bfloat16)


def score_tile(kq_ref, pc_ref, query_low, q_base, u_base, u_rows):
    q_rows = query_low.shape[0]
    shift = pc_ref[q_base : q_base + 1, :] - pc_ref[u_base : u_base + u_rows]
    shift = jnp.concatenate([shift] * (q_rows // LANES), axis=1)
    scores = dot_nt(kq_ref[u_base : u_base + u_rows], query_low) + shift
    if u_base != q_base:
        return scores
    place = lax.broadcasted_iota(jnp.int32, scores.shape, 0)
    seen = place <= lax.broadcasted_iota(jnp.int32, scores.shape, 1)
    return jnp.where(seen, scores, FLOOR)


def stats_kernel(x_ref, p_ref, peak_ref, share_ref, kq_ref, pc_ref, s_ref):
    blocks = blocks_of(x_ref.shape[0])
    spread(x_ref, p_ref, kq_ref, pc_ref)
    for index, (q_base, q_rows) in enumerate(blocks):
        q_here = slice(q_base, q_base + q_rows)
        query_low, _ = query_block(x_ref, q_here, low_lanes((q_rows, LANES)))
        peak = jnp.full((8, q_rows), FLOOR, jnp.float32)
        for u_base, u_rows in blocks[: index + 1]:
            scores = score_tile(kq_ref, pc_ref, query_low, q_base, u_base, u_rows)
            s_ref[u_base : u_base + u_rows, :q_rows] = scores
            peak = jnp.maximum(peak, folded(scores, jnp.max))
        peak = jnp.max(peak, axis=0, keepdims=True)
        total = jnp.zeros((8, q_rows), jnp.float32)
        for u_base, u_rows in blocks[: index + 1]:
            raised = jnp.exp(s_ref[u_base : u_base + u_rows, :q_rows] - peak)
            total = total + folded(raised, jnp.sum)
        peak_ref[:, q_here] = peak
        share_ref[:, q_here] = 1.0 / jnp.sum(total, axis=0, keepdims=True)


def value_kernel(x_ref, y_ref, p_ref, peak_ref, share_ref, v_out_ref, kq_ref, pc_ref, acc_ref):
    length = x_ref.shape[0]
    blocks = blocks_of(length)
    spread(x_ref, p_ref, kq_ref, pc_ref, acc_ref)
    for index, (q_base, q_rows) in enumerate(blocks):
        q_here = slice(q_base, q_base + q_rows)
        low = low_lanes((q_rows, LANES))
        query_low, _ = query_block(x_ref, q_here, low)
        grad_low = grad_block(y_ref, q_here, low)
        peak = peak_ref[:, q_here]
        share = share_ref[:, q_here]
        for u_base, u_rows in blocks[: index + 1]:
            scores = score_tile(kq_ref, pc_ref, query_low, q_base, u_base, u_rows)
            soft = (jnp.exp(scores - peak) * share).astype(jnp.bfloat16)
            acc_ref[u_base : u_base + u_rows] += dot_nn(soft, grad_low)
    planes, kept, _ = v_out_ref.shape
    tokens = length // planes
    for plane in range(planes):
        base = plane * tokens
        first = acc_ref[base : base + kept]
        second = acc_ref[base + kept : base + tokens]
        second = jnp.concatenate([second, first[: 2 * kept - tokens]], axis=0)
        v_out_ref[plane] = jnp.where(low_lanes(first.shape), first, rolled(second)).astype(
            jnp.bfloat16
        )


def pair_kernel(
    x_ref, y_ref, p_ref, peak_ref, share_ref, qk_ref, kq_ref, kt_ref, pc_ref, acc_ref, s_ref, d_ref
):
    blocks = blocks_of(x_ref.shape[0])
    scale = HEAD_DIM**-0.5
    spread(x_ref, p_ref, kq_ref, pc_ref, acc_ref, kt_ref)
    for index, (q_base, q_rows) in enumerate(blocks):
        q_here = slice(q_base, q_base + q_rows)
        low = low_lanes((q_rows, LANES))
        query_low, query_high = query_block(x_ref, q_here, low)
        grad_low = grad_block(y_ref, q_here, low)
        peak = peak_ref[:, q_here]
        share = share_ref[:, q_here]
        term = jnp.zeros((8, q_rows), jnp.float32)
        for u_base, u_rows in blocks[: index + 1]:
            u_here = slice(u_base, u_base + u_rows)
            scores = score_tile(kq_ref, pc_ref, query_low, q_base, u_base, u_rows)
            soft = jnp.exp(scores - peak) * share
            s_ref[u_here, :q_rows] = soft
            soft_grad = dot_nt(y_ref[u_here], grad_low)
            d_ref[u_here, :q_rows] = soft_grad
            term = term + folded(soft * soft_grad, jnp.sum)
        term = jnp.sum(term, axis=0, keepdims=True)
        query_grad = jnp.zeros((HEAD_DIM, q_rows), jnp.float32)
        for u_base, u_rows in blocks[: index + 1]:
            u_here = slice(u_base, u_base + u_rows)
            score_low = (s_ref[u_here, :q_rows] * (d_ref[u_here, :q_rows] - term)).astype(
                jnp.bfloat16
            )
            acc_ref[u_here] += dot_nn(score_low, query_high)
            query_grad = query_grad + dot_nn(kt_ref[:, u_here], score_low)
        query_grad = jnp.concatenate([query_grad, jnp.zeros_like(query_grad)], axis=0)
        acc_ref[q_here] += query_grad.T
    for base, rows in blocks:
        here = slice(base, base + rows)
        qk_ref[here] = (acc_ref[here] * scale).astype(jnp.bfloat16)


def unpack_value_kernel(place_ref, x_ref, mine_ref, away_ref):
    heads, kept, _ = x_ref.shape
    columns, tokens, _ = mine_ref.shape
    rest = tokens - kept
    cores = HEAD_DIM * columns // LANES
    quarter = HEAD_DIM // cores
    lane = lax.broadcasted_iota(jnp.int32, (tokens, LANES), 1)
    first_core = place_ref[0] == 0
    for column in range(columns):
        step = (column + columns - place_ref[1]) % columns
        parts = [jnp.zeros((tokens, LANES), jnp.float32)] * cores
        for group in range(heads // columns):
            block = x_ref[group * columns + column].astype(jnp.float32)
            for core in range(cores):
                home = group * quarter
                top = pltpu.roll(block, (home - core * quarter) % LANES, 1)
                bottom = pltpu.roll(block, (home - core * quarter - HEAD_DIM) % LANES, 1)[:rest]
                moved = jnp.concatenate([top, bottom], axis=0)
                inside = (lane >= home) & (lane < home + quarter)
                parts[core] = jnp.where(inside, moved, parts[core])
        mine_ref[step] = jnp.where(first_core, parts[0], parts[1]).astype(jnp.bfloat16)
        away_ref[step] = jnp.where(first_core, parts[1], parts[0]).astype(jnp.bfloat16)


def weight_line_kernel(place_ref, *refs):
    pieces, out_ref = refs[:-1], refs[-1]
    lines = out_ref.shape[0]
    for step, piece_ref in enumerate(pieces):
        out_ref[(place_ref[1] + lines - step) % lines] = piece_ref[...]


def stack_kernel(*refs):
    for step, piece_ref in enumerate(refs[:-1]):
        refs[-1][step] = piece_ref[...]


def dot_tn(a, b):
    return lax.dot_general(a, b, (((0,), (0,)), ((), ())), preferred_element_type=jnp.float32)


def product_kernel(place_ref, own_ref, other_ref, *refs):
    columns = own_ref.shape[0]
    pieces, (block_ref,) = refs[:columns], refs[-1:]
    outs = refs[columns:-1]
    lines, w_cols, model = block_ref.shape
    width = 4 * LANES
    own = jnp.concatenate([piece[0] for piece in pieces], axis=0)
    other = jnp.concatenate([piece[1] for piece in pieces], axis=0)
    rows = own.shape[0]
    for base in range(0, model, width):
        cols = slice(base, base + width)
        total = dot_tn(own, own_ref[:, :, cols].reshape(rows, width))
        total = total + dot_tn(other, other_ref[:, :, cols].reshape(rows, width))
        block_ref[:, :, cols] = total.astype(jnp.bfloat16).reshape(lines, w_cols, width)
    for step, out_ref in enumerate(outs):
        out_ref[...] = block_ref[(place_ref[2] + step) % lines]


def input_grad_kernel(place_ref, first_ref, second_ref, *refs):
    columns, tokens, _ = first_ref.shape
    weight_ref = refs[-1]
    mine_ref, away_ref = refs[-3:-1]
    lines, w_cols = weight_ref.shape[1:3]
    for step, piece_ref in enumerate(refs[:-3]):
        for column in range(columns):
            weight_ref[column, (place_ref[2] + lines - step) % lines] = piece_ref[
                column * w_cols : (column + 1) * w_cols
            ]
    width = 4 * LANES
    for base in range(0, mine_ref.shape[1], width):
        cols = slice(base, base + width)
        first = jnp.zeros((tokens, width), jnp.float32)
        second = jnp.zeros((tokens, width), jnp.float32)
        for step in range(columns):
            weight = weight_ref[(place_ref[1] + step) % columns, :, :, cols]
            weight = weight.reshape(LANES, width)
            first = first + dot_nn(first_ref[step], weight)
            second = second + dot_nn(second_ref[step], weight)
        mine_ref[:, cols] = first
        away_ref[:, cols] = second.astype(jnp.bfloat16)


def add_kernel(first_ref, second_ref, out_ref):
    total = first_ref[...] + second_ref[...].astype(jnp.float32)
    out_ref[...] = total.astype(jnp.bfloat16)


def unpack_pair_kernel(x_ref, q_ref, k_ref):
    heads, tokens, _ = x_ref.shape
    low = low_lanes((tokens, LANES))
    for pair in range(heads // 2):
        first = x_ref[2 * pair].astype(jnp.float32)
        second = x_ref[2 * pair + 1].astype(jnp.float32)
        cols = slice(pair * LANES, (pair + 1) * LANES)
        q_ref[:, cols] = jnp.where(low, first, rolled(second)).astype(jnp.bfloat16)
        k_ref[:, cols] = jnp.where(low, rolled(first), second).astype(jnp.bfloat16)


def exchanged(x, axis):
    return lax.all_to_all(x, axis, split_axis=0, concat_axis=0, tiled=True)


def shifted(x, axis, step):
    count = lax.axis_size(axis)
    return lax.ppermute(x, axis, [(place, (place + step) % count) for place in range(count)])


def from_all(x, axis):
    return [x] + [shifted(x, axis, step) for step in range(1, lax.axis_size(axis))]


def near(x):
    return pltpu.with_memory_space_constraint(x, pltpu.VMEM)


def shaped(*shape, dtype=jnp.bfloat16):
    return jax.ShapeDtypeStruct(shape, dtype)


def shards(inputs, query_vectors, key_vectors, value_vectors, cotangent, gate_prefix, value_weight):
    planes = lax.axis_size("sp")
    columns, lines = lax.axis_size("x"), lax.axis_size("y")
    core = lax.axis_index("core")
    tokens, model = inputs.shape[1:]
    width = query_vectors.shape[2]
    heads = width // HEAD_DIM
    length = planes * tokens
    w_cols = value_weight.shape[1]
    place = jnp.stack([core, lax.axis_index("x"), lax.axis_index("y")]).astype(jnp.int32)
    small, whole = pl.BlockSpec(memory_space=pltpu.SMEM), pl.BlockSpec(memory_space=pltpu.VMEM)
    first, second = pl.pallas_call(
        pack_kernel,
        out_shape=(shaped(heads, tokens + w_cols, LANES), shaped(heads, tokens, LANES)),
    )(query_vectors[0], key_vectors[0], value_vectors[0], cotangent[0], value_weight.T)
    first = exchanged(first, "sp")
    second = near(exchanged(second, "sp").reshape(length, LANES))
    sequence, weight_block = pl.pallas_call(
        open_kernel, out_shape=(shaped(planes, tokens, LANES), shaped(w_cols, model))
    )(near(first))
    sequence = sequence.reshape(length, LANES)
    own_rows = pl.pallas_call(stack_kernel, out_shape=shaped(columns, tokens, model))(
        inputs[0], *map(near, from_all(inputs[0], "x")[1:])
    )
    other_rows = shifted(own_rows, "core", 1)
    weight_line = pl.pallas_call(
        weight_line_kernel,
        out_shape=shaped(columns, w_cols, model),
        in_specs=[small] + [whole] * columns,
    )(place, weight_block, *map(near, from_all(weight_block, "x")[1:]))
    weight_line = weight_line.reshape(columns * w_cols, model)
    weight_pieces = from_all(weight_line, "y")
    kept = (tokens // 2 + 7) // 8 * 8
    wide, tile = pltpu.VMEM((length, LANES), jnp.float32), pltpu.VMEM((length, TILE), jnp.float32)
    swapped = pltpu.VMEM((length, LANES), jnp.bfloat16)
    row = shaped(1, length, dtype=jnp.float32)
    peak, share = pl.pallas_call(
        stats_kernel, out_shape=(row, row), scratch_shapes=[swapped, wide, tile]
    )(sequence, gate_prefix[0])
    value_grad = pl.pallas_call(
        value_kernel,
        out_shape=shaped(planes, kept, LANES),
        scratch_shapes=[swapped, wide, wide],
    )(sequence, second, gate_prefix[0], peak, share)
    value_back = exchanged(value_grad, "sp")
    pair_grad = pl.pallas_call(
        pair_kernel,
        out_shape=shaped(length, LANES),
        scratch_shapes=[
            pltpu.VMEM((length, LANES), jnp.bfloat16),
            pltpu.VMEM((HEAD_DIM, length), jnp.bfloat16),
            wide,
            wide,
            tile,
            tile,
        ],
    )(sequence, second, gate_prefix[0], peak, share)
    pair_back = exchanged(pair_grad.reshape(planes, tokens, LANES), "sp")
    block = shaped(columns, tokens, LANES)
    mine, away = pl.pallas_call(
        unpack_value_kernel, out_shape=(block, block), in_specs=[small, whole]
    )(place, near(value_back))
    brought = shifted(away, "core", 1)
    both = jnp.stack([mine, brought], axis=1)
    pieces = [both[0]] + [shifted(both[step], "x", step) for step in range(1, columns)]
    partial = pl.pallas_call(
        product_kernel,
        compiler_params=pltpu.CompilerParams(vmem_limit_bytes=VMEM_BYTES),
        out_shape=(shaped(w_cols, model),) * lines,
        in_specs=[small] + [whole] * (2 + columns),
        scratch_shapes=[pltpu.VMEM((lines, w_cols, model), jnp.bfloat16)],
    )(place, near(own_rows), near(other_rows), *map(near, pieces))
    partial = [partial[0]] + [shifted(partial[step], "y", step) for step in range(1, lines)]
    partial = sum(part.astype(jnp.float32) for part in partial).astype(jnp.bfloat16)
    partial = jnp.moveaxis(partial.reshape(w_cols, planes, model // planes), 1, 0)
    partial = exchanged(partial, "sp")
    weight_grad = partial.astype(jnp.float32).sum(axis=0).T
    query_grad, key_grad = pl.pallas_call(
        unpack_pair_kernel, out_shape=(shaped(tokens, width), shaped(tokens, width))
    )(near(pair_back))
    kept_part, sent_part = pl.pallas_call(
        input_grad_kernel,
        out_shape=(shaped(tokens, model, dtype=jnp.float32), shaped(tokens, model)),
        in_specs=[small] + [whole] * (2 + lines),
        scratch_shapes=[pltpu.VMEM((columns, lines, w_cols, model), jnp.bfloat16)],
    )(place, mine, near(brought), *weight_pieces)
    input_grad = pl.pallas_call(add_kernel, out_shape=shaped(tokens, model))(
        kept_part, near(shifted(sent_part, "core", 1))
    )
    return (query_grad[None], key_grad[None], input_grad[None], weight_grad)


def solution(mesh):
    grid = Mesh(mesh.devices.reshape(-1, 4, 4, 2), ("sp", "y", "x", "core"))
    rows = P(("y", "x", "core"), "sp", None)
    weight = P("sp", ("y", "x", "core"))

    return jax.shard_map(
        shards,
        mesh=grid,
        in_specs=(rows,) * 6 + (weight,),
        out_specs=(rows, rows, rows, weight),
        check_vma=False,
    )
```

```python
import jax
import jax.numpy as jnp
from jax import lax
from jax.experimental import pallas as pl
from jax.experimental.pallas import tpu as pltpu
from jax.sharding import Mesh, PartitionSpec as P

HEAD_DIM = 64
LANES = 128
TILE = 256
FLOOR = -1e30
VMEM_BYTES = 24 * 1024 * 1024


def rolled(x):
    return pltpu.roll(x, HEAD_DIM, 1)


def low_lanes(shape):
    return lax.broadcasted_iota(jnp.int32, shape, 1) < HEAD_DIM


def pack_kernel(q_ref, k_ref, v_ref, g_ref, out_ref):
    heads, tokens, _ = out_ref.shape
    low = low_lanes((tokens, LANES))
    for pair in range(heads // 2):
        cols = slice(pair * LANES, (pair + 1) * LANES)
        for first_ref, second_ref, lane in ((q_ref, k_ref, 0), (v_ref, g_ref, LANES)):
            first = first_ref[:, cols].astype(jnp.float32)
            second = second_ref[:, cols].astype(jnp.float32)
            out_ref[2 * pair, :, lane : lane + LANES] = jnp.where(
                low, first, rolled(second)
            ).astype(jnp.bfloat16)
            out_ref[2 * pair + 1, :, lane : lane + LANES] = jnp.where(
                low, rolled(first), second
            ).astype(jnp.bfloat16)


def dot_nt(a, b):
    return lax.dot_general(a, b, (((1,), (1,)), ((), ())), preferred_element_type=jnp.float32)


def dot_nn(a, b):
    return lax.dot_general(a, b, (((1,), (0,)), ((), ())), preferred_element_type=jnp.float32)


def folded(x, op):
    return op(x.reshape(x.shape[0] // 8, 8, x.shape[1]), axis=0)


def attention_kernel(
    x_ref, p_ref, qk_ref, v_out_ref, kq_ref, kt_ref, pc_ref, acc_ref, dq_ref, s_ref, d_ref
):
    length = x_ref.shape[0]
    scale = HEAD_DIM**-0.5
    blocks = [(b, min(TILE, length - b)) for b in range(0, length, TILE)]
    for base, rows in blocks:
        here = slice(base, base + rows)
        wide = x_ref[here, :LANES].astype(jnp.float32)
        swapped = rolled(wide)
        kq_ref[here] = swapped.astype(jnp.bfloat16)
        kt_ref[:, here] = swapped.T[:HEAD_DIM].astype(jnp.bfloat16)
        pc_ref[here] = jnp.broadcast_to(p_ref[:, here], (LANES, rows)).T
        acc_ref[here] = jnp.zeros((rows, LANES), jnp.float32)
    for index, (q_base, q_rows) in enumerate(blocks):
        q_here = slice(q_base, q_base + q_rows)
        low = low_lanes((q_rows, LANES))
        query_wide = x_ref[q_here, :LANES].astype(jnp.float32)
        grad_wide = rolled(x_ref[q_here, LANES:].astype(jnp.float32))
        query_low = jnp.where(low, query_wide * scale, 0.0).astype(jnp.bfloat16)
        query_high = jnp.where(low, 0.0, rolled(query_wide)).astype(jnp.bfloat16)
        grad_low = jnp.where(low, grad_wide, 0.0).astype(jnp.bfloat16)
        pivot = pc_ref[q_base : q_base + 1, :]
        peak = jnp.full((8, q_rows), FLOOR, jnp.float32)
        for u_base, u_rows in blocks[: index + 1]:
            u_here = slice(u_base, u_base + u_rows)
            shift = pivot - pc_ref[u_here]
            shift = jnp.concatenate([shift] * (q_rows // LANES), axis=1)
            scores = dot_nt(kq_ref[u_here], query_low) + shift
            if u_base == q_base:
                seen = lax.broadcasted_iota(jnp.int32, scores.shape, 0) <= lax.broadcasted_iota(
                    jnp.int32, scores.shape, 1
                )
                scores = jnp.where(seen, scores, FLOOR)
            s_ref[u_here, :q_rows] = scores
            peak = jnp.maximum(peak, folded(scores, jnp.max))
        peak = jnp.max(peak, axis=0, keepdims=True)
        total = jnp.zeros((8, q_rows), jnp.float32)
        for u_base, u_rows in blocks[: index + 1]:
            u_here = slice(u_base, u_base + u_rows)
            raised = jnp.exp(s_ref[u_here, :q_rows] - peak)
            s_ref[u_here, :q_rows] = raised
            total = total + folded(raised, jnp.sum)
        share = 1.0 / jnp.sum(total, axis=0, keepdims=True)
        term = jnp.zeros((8, q_rows), jnp.float32)
        for u_base, u_rows in blocks[: index + 1]:
            u_here = slice(u_base, u_base + u_rows)
            soft = s_ref[u_here, :q_rows] * share
            s_ref[u_here, :q_rows] = soft
            acc_ref[u_here] += dot_nn(soft.astype(jnp.bfloat16), grad_low)
            soft_grad = dot_nt(x_ref[u_here, LANES:], grad_low)
            d_ref[u_here, :q_rows] = soft_grad
            term = term + folded(soft * soft_grad, jnp.sum)
        term = jnp.sum(term, axis=0, keepdims=True)
        query_grad = jnp.zeros((HEAD_DIM, q_rows), jnp.float32)
        for u_base, u_rows in blocks[: index + 1]:
            u_here = slice(u_base, u_base + u_rows)
            score_low = (s_ref[u_here, :q_rows] * (d_ref[u_here, :q_rows] - term)).astype(
                jnp.bfloat16
            )
            acc_ref[u_here] += dot_nn(score_low, query_high)
            query_grad = query_grad + dot_nn(kt_ref[:, u_here], score_low)
        query_grad = jnp.concatenate([query_grad, jnp.zeros_like(query_grad)], axis=0)
        dq_ref[q_here] = query_grad.T
    for base, rows in blocks:
        here = slice(base, base + rows)
        qk_ref[here] = (
            jnp.where(low_lanes((rows, LANES)), dq_ref[here], acc_ref[here]) * scale
        ).astype(jnp.bfloat16)
    planes, kept, _ = v_out_ref.shape
    tokens = length // planes
    for plane in range(planes):
        base = plane * tokens
        first = acc_ref[base : base + kept]
        second = acc_ref[base + kept : base + tokens]
        second = jnp.concatenate([second, first[: 2 * kept - tokens]], axis=0)
        v_out_ref[plane] = jnp.where(low_lanes(first.shape), first, rolled(second)).astype(
            jnp.bfloat16
        )


def spread_kernel(w_ref, out_ref):
    for plane in range(out_ref.shape[0]):
        out_ref[plane] = w_ref[...]


def unpack_value_kernel(place_ref, x_ref, mine_ref, away_ref):
    heads, kept, _ = x_ref.shape
    columns, tokens, _ = mine_ref.shape
    rest = tokens - kept
    cores = HEAD_DIM * columns // LANES
    quarter = HEAD_DIM // cores
    lane = lax.broadcasted_iota(jnp.int32, (tokens, LANES), 1)
    first_core = place_ref[0] == 0
    for column in range(columns):
        step = (column + columns - place_ref[1]) % columns
        parts = [jnp.zeros((tokens, LANES), jnp.float32)] * cores
        for group in range(heads // columns):
            block = x_ref[group * columns + column].astype(jnp.float32)
            for core in range(cores):
                home = group * quarter
                top = pltpu.roll(block, (home - core * quarter) % LANES, 1)
                bottom = pltpu.roll(block, (home - core * quarter - HEAD_DIM) % LANES, 1)[:rest]
                moved = jnp.concatenate([top, bottom], axis=0)
                inside = (lane >= home) & (lane < home + quarter)
                parts[core] = jnp.where(inside, moved, parts[core])
        mine_ref[step] = jnp.where(first_core, parts[0], parts[1]).astype(jnp.bfloat16)
        away_ref[step] = jnp.where(first_core, parts[1], parts[0]).astype(jnp.bfloat16)


def weight_open_kernel(x_ref, out_ref):
    for plane in range(x_ref.shape[0]):
        out_ref[:, plane * LANES : (plane + 1) * LANES] = x_ref[plane]


def weight_line_kernel(place_ref, *refs):
    pieces, out_ref = refs[:-1], refs[-1]
    lines = out_ref.shape[0]
    for step, piece_ref in enumerate(pieces):
        out_ref[(place_ref[1] + lines - step) % lines] = piece_ref[...]


def stack_kernel(*refs):
    for step, piece_ref in enumerate(refs[:-1]):
        refs[-1][step] = piece_ref[...]


def dot_tn(a, b):
    return lax.dot_general(a, b, (((0,), (0,)), ((), ())), preferred_element_type=jnp.float32)


def product_kernel(place_ref, own_ref, other_ref, *refs):
    columns = own_ref.shape[0]
    pieces, (block_ref,) = refs[:columns], refs[-1:]
    outs = refs[columns:-1]
    lines, w_cols, model = block_ref.shape
    width = 4 * LANES
    own = jnp.concatenate([piece[0] for piece in pieces], axis=0)
    other = jnp.concatenate([piece[1] for piece in pieces], axis=0)
    rows = own.shape[0]
    for base in range(0, model, width):
        cols = slice(base, base + width)
        total = dot_tn(own, own_ref[:, :, cols].reshape(rows, width))
        total = total + dot_tn(other, other_ref[:, :, cols].reshape(rows, width))
        block_ref[:, :, cols] = total.astype(jnp.bfloat16).reshape(lines, w_cols, width)
    for step, out_ref in enumerate(outs):
        out_ref[...] = block_ref[(place_ref[2] + step) % lines]


def input_grad_kernel(place_ref, first_ref, second_ref, *refs):
    columns, tokens, _ = first_ref.shape
    weight_ref = refs[-1]
    mine_ref, away_ref = refs[-3:-1]
    lines, w_cols = weight_ref.shape[1:3]
    for step, piece_ref in enumerate(refs[:-3]):
        for column in range(columns):
            weight_ref[column, (place_ref[2] + lines - step) % lines] = piece_ref[
                column * w_cols : (column + 1) * w_cols
            ]
    width = 4 * LANES
    for base in range(0, mine_ref.shape[1], width):
        cols = slice(base, base + width)
        first = jnp.zeros((tokens, width), jnp.float32)
        second = jnp.zeros((tokens, width), jnp.float32)
        for step in range(columns):
            weight = weight_ref[(place_ref[1] + step) % columns, :, :, cols]
            weight = weight.reshape(LANES, width)
            first = first + dot_nn(first_ref[step], weight)
            second = second + dot_nn(second_ref[step], weight)
        mine_ref[:, cols] = first
        away_ref[:, cols] = second.astype(jnp.bfloat16)


def add_kernel(first_ref, second_ref, out_ref):
    total = first_ref[...] + second_ref[...].astype(jnp.float32)
    out_ref[...] = total.astype(jnp.bfloat16)


def unpack_pair_kernel(x_ref, q_ref, k_ref):
    heads, tokens, _ = x_ref.shape
    low = low_lanes((tokens, LANES))
    for pair in range(heads // 2):
        first = x_ref[2 * pair].astype(jnp.float32)
        second = x_ref[2 * pair + 1].astype(jnp.float32)
        cols = slice(pair * LANES, (pair + 1) * LANES)
        q_ref[:, cols] = jnp.where(low, first, rolled(second)).astype(jnp.bfloat16)
        k_ref[:, cols] = jnp.where(low, rolled(first), second).astype(jnp.bfloat16)


def exchanged(x, axis):
    return lax.all_to_all(x, axis, split_axis=0, concat_axis=0, tiled=True)


def shifted(x, axis, step):
    count = lax.axis_size(axis)
    return lax.ppermute(x, axis, [(place, (place + step) % count) for place in range(count)])


def from_all(x, axis):
    return [x] + [shifted(x, axis, step) for step in range(1, lax.axis_size(axis))]


def near(x):
    return pltpu.with_memory_space_constraint(x, pltpu.VMEM)


def shaped(*shape, dtype=jnp.bfloat16):
    return jax.ShapeDtypeStruct(shape, dtype)


def shards(inputs, query_vectors, key_vectors, value_vectors, cotangent, gate_prefix, value_weight):
    planes = lax.axis_size("sp")
    columns, lines = lax.axis_size("x"), lax.axis_size("y")
    core = lax.axis_index("core")
    tokens, model = inputs.shape[1:]
    width = query_vectors.shape[2]
    heads = width // HEAD_DIM
    length = planes * tokens
    w_cols = value_weight.shape[1]
    place = jnp.stack([core, lax.axis_index("x"), lax.axis_index("y")]).astype(jnp.int32)
    small, whole = pl.BlockSpec(memory_space=pltpu.SMEM), pl.BlockSpec(memory_space=pltpu.VMEM)
    packed = pl.pallas_call(pack_kernel, out_shape=shaped(heads, tokens, 2 * LANES))(
        query_vectors[0], key_vectors[0], value_vectors[0], cotangent[0]
    )
    arrived = exchanged(packed, "sp")
    weight_block = pl.pallas_call(
        spread_kernel, out_shape=shaped(planes, w_cols, model // planes)
    )(value_weight.T)
    weight_block = exchanged(weight_block, "sp")
    weight_block = pl.pallas_call(weight_open_kernel, out_shape=shaped(w_cols, model))(
        near(weight_block)
    )
    own_rows = pl.pallas_call(stack_kernel, out_shape=shaped(columns, tokens, model))(
        inputs[0], *map(near, from_all(inputs[0], "x")[1:])
    )
    other_rows = shifted(own_rows, "core", 1)
    weight_line = pl.pallas_call(
        weight_line_kernel,
        out_shape=shaped(columns, w_cols, model),
        in_specs=[small] + [whole] * columns,
    )(place, weight_block, *map(near, from_all(weight_block, "x")[1:]))
    weight_line = weight_line.reshape(columns * w_cols, model)
    weight_pieces = [weight_line]
    for step in range(1, lines):
        weight_pieces.append(shifted(weight_line, "y", step))
    kept = (tokens // 2 + 7) // 8 * 8
    sequence = near(arrived.reshape(length, 2 * LANES))
    wide, tile = pltpu.VMEM((length, LANES), jnp.float32), pltpu.VMEM((length, TILE), jnp.float32)
    pair_grad, value_grad = pl.pallas_call(
        attention_kernel,
        out_shape=(shaped(length, LANES), shaped(planes, kept, LANES)),
        scratch_shapes=[
            pltpu.VMEM((length, LANES), jnp.bfloat16),
            pltpu.VMEM((HEAD_DIM, length), jnp.bfloat16),
            wide,
            wide,
            wide,
            tile,
            tile,
        ],
    )(sequence, gate_prefix[0])
    value_back = exchanged(value_grad, "sp")
    pair_back = exchanged(pair_grad.reshape(planes, tokens, LANES), "sp")
    block = shaped(columns, tokens, LANES)
    mine, away = pl.pallas_call(
        unpack_value_kernel, out_shape=(block, block), in_specs=[small, whole]
    )(place, near(value_back))
    brought = shifted(away, "core", 1)
    both = jnp.stack([mine, brought], axis=1)
    pieces = [both[0]] + [shifted(both[step], "x", step) for step in range(1, columns)]
    partial = pl.pallas_call(
        product_kernel,
        compiler_params=pltpu.CompilerParams(vmem_limit_bytes=VMEM_BYTES),
        out_shape=(shaped(w_cols, model),) * lines,
        in_specs=[small] + [whole] * (2 + columns),
        scratch_shapes=[pltpu.VMEM((lines, w_cols, model), jnp.bfloat16)],
    )(place, near(own_rows), near(other_rows), *map(near, pieces))
    partial = [partial[0]] + [shifted(partial[step], "y", step) for step in range(1, lines)]
    partial = sum(part.astype(jnp.float32) for part in partial).astype(jnp.bfloat16)
    partial = jnp.moveaxis(partial.reshape(w_cols, planes, model // planes), 1, 0)
    partial = exchanged(partial, "sp")
    weight_grad = partial.astype(jnp.float32).sum(axis=0).T
    query_grad, key_grad = pl.pallas_call(
        unpack_pair_kernel, out_shape=(shaped(tokens, width), shaped(tokens, width))
    )(near(pair_back))
    kept_part, sent_part = pl.pallas_call(
        input_grad_kernel,
        out_shape=(shaped(tokens, model, dtype=jnp.float32), shaped(tokens, model)),
        in_specs=[small] + [whole] * (2 + lines),
        scratch_shapes=[pltpu.VMEM((columns, lines, w_cols, model), jnp.bfloat16)],
    )(place, mine, near(brought), *weight_pieces)
    input_grad = pl.pallas_call(add_kernel, out_shape=shaped(tokens, model))(
        kept_part, near(shifted(sent_part, "core", 1))
    )
    return (query_grad[None], key_grad[None], input_grad[None], weight_grad)


def solution(mesh):
    grid = Mesh(mesh.devices.reshape(-1, 4, 4, 2), ("sp", "y", "x", "core"))
    rows = P(("y", "x", "core"), "sp", None)
    weight = P("sp", ("y", "x", "core"))

    return jax.shard_map(
        shards,
        mesh=grid,
        in_specs=(rows,) * 6 + (weight,),
        out_specs=(rows, rows, rows, weight),
        check_vma=False,
    )
```

```python
import jax
import jax.numpy as jnp
from jax import lax
from jax.experimental import pallas as pl
from jax.experimental.pallas import tpu as pltpu
from jax.sharding import Mesh, PartitionSpec as P

HEAD_DIM = 64
LANES = 128
TILE = 256
FLOOR = -1e30
VMEM_BYTES = 24 * 1024 * 1024


def rolled(x):
    return pltpu.roll(x, HEAD_DIM, 1)


def low_lanes(shape):
    return lax.broadcasted_iota(jnp.int32, shape, 1) < HEAD_DIM


def pack_kernel(q_ref, k_ref, v_ref, g_ref, out_ref):
    heads, tokens, _ = out_ref.shape
    low = low_lanes((tokens, LANES))
    for pair in range(heads // 2):
        cols = slice(pair * LANES, (pair + 1) * LANES)
        for first_ref, second_ref, lane in ((q_ref, k_ref, 0), (v_ref, g_ref, LANES)):
            first = first_ref[:, cols].astype(jnp.float32)
            second = second_ref[:, cols].astype(jnp.float32)
            out_ref[2 * pair, :, lane : lane + LANES] = jnp.where(
                low, first, rolled(second)
            ).astype(jnp.bfloat16)
            out_ref[2 * pair + 1, :, lane : lane + LANES] = jnp.where(
                low, rolled(first), second
            ).astype(jnp.bfloat16)


def dot_nt(a, b):
    return lax.dot_general(a, b, (((1,), (1,)), ((), ())), preferred_element_type=jnp.float32)


def dot_nn(a, b):
    return lax.dot_general(a, b, (((1,), (0,)), ((), ())), preferred_element_type=jnp.float32)


def folded(x, op):
    return op(x.reshape(x.shape[0] // 8, 8, x.shape[1]), axis=0)


def blocks_of(length):
    return [(base, min(TILE, length - base)) for base in range(0, length, TILE)]


def spread(x_ref, p_ref, kq_ref, pc_ref, acc_ref, kt_ref=None):
    for base, rows in blocks_of(x_ref.shape[0]):
        here = slice(base, base + rows)
        swapped = rolled(x_ref[here, :LANES].astype(jnp.float32))
        kq_ref[here] = swapped.astype(jnp.bfloat16)
        if kt_ref is not None:
            kt_ref[:, here] = swapped.T[:HEAD_DIM].astype(jnp.bfloat16)
        pc_ref[here] = jnp.broadcast_to(p_ref[:, here], (LANES, rows)).T
        acc_ref[here] = jnp.zeros((rows, LANES), jnp.float32)


def query_block(x_ref, here, low):
    wide = x_ref[here, :LANES].astype(jnp.float32)
    scaled = jnp.where(low, wide * HEAD_DIM**-0.5, 0.0).astype(jnp.bfloat16)
    return scaled, jnp.where(low, 0.0, rolled(wide)).astype(jnp.bfloat16)


def grad_block(x_ref, here, low):
    wide = rolled(x_ref[here, LANES:].astype(jnp.float32))
    return jnp.where(low, wide, 0.0).astype(jnp.bfloat16)


def score_tile(kq_ref, pc_ref, query_low, q_base, u_base, u_rows):
    q_rows = query_low.shape[0]
    shift = pc_ref[q_base : q_base + 1, :] - pc_ref[u_base : u_base + u_rows]
    shift = jnp.concatenate([shift] * (q_rows // LANES), axis=1)
    scores = dot_nt(kq_ref[u_base : u_base + u_rows], query_low) + shift
    if u_base != q_base:
        return scores
    place = lax.broadcasted_iota(jnp.int32, scores.shape, 0)
    seen = place <= lax.broadcasted_iota(jnp.int32, scores.shape, 1)
    return jnp.where(seen, scores, FLOOR)


def value_kernel(x_ref, p_ref, v_out_ref, peak_ref, share_ref, kq_ref, pc_ref, acc_ref, s_ref):
    length = x_ref.shape[0]
    blocks = blocks_of(length)
    spread(x_ref, p_ref, kq_ref, pc_ref, acc_ref)
    for index, (q_base, q_rows) in enumerate(blocks):
        q_here = slice(q_base, q_base + q_rows)
        low = low_lanes((q_rows, LANES))
        query_low, _ = query_block(x_ref, q_here, low)
        grad_low = grad_block(x_ref, q_here, low)
        peak = jnp.full((8, q_rows), FLOOR, jnp.float32)
        for u_base, u_rows in blocks[: index + 1]:
            scores = score_tile(kq_ref, pc_ref, query_low, q_base, u_base, u_rows)
            s_ref[u_base : u_base + u_rows, :q_rows] = scores
            peak = jnp.maximum(peak, folded(scores, jnp.max))
        peak = jnp.max(peak, axis=0, keepdims=True)
        total = jnp.zeros((8, q_rows), jnp.float32)
        for u_base, u_rows in blocks[: index + 1]:
            u_here = slice(u_base, u_base + u_rows)
            raised = jnp.exp(s_ref[u_here, :q_rows] - peak)
            s_ref[u_here, :q_rows] = raised
            total = total + folded(raised, jnp.sum)
        share = 1.0 / jnp.sum(total, axis=0, keepdims=True)
        peak_ref[:, q_here] = peak
        share_ref[:, q_here] = share
        for u_base, u_rows in blocks[: index + 1]:
            u_here = slice(u_base, u_base + u_rows)
            soft = s_ref[u_here, :q_rows] * share
            acc_ref[u_here] += dot_nn(soft.astype(jnp.bfloat16), grad_low)
    planes, kept, _ = v_out_ref.shape
    tokens = length // planes
    for plane in range(planes):
        base = plane * tokens
        first = acc_ref[base : base + kept]
        second = acc_ref[base + kept : base + tokens]
        second = jnp.concatenate([second, first[: 2 * kept - tokens]], axis=0)
        v_out_ref[plane] = jnp.where(low_lanes(first.shape), first, rolled(second)).astype(
            jnp.bfloat16
        )


def pair_kernel(
    x_ref, p_ref, peak_ref, share_ref, qk_ref, kq_ref, kt_ref, pc_ref, acc_ref, s_ref, d_ref
):
    blocks = blocks_of(x_ref.shape[0])
    scale = HEAD_DIM**-0.5
    spread(x_ref, p_ref, kq_ref, pc_ref, acc_ref, kt_ref)
    for index, (q_base, q_rows) in enumerate(blocks):
        q_here = slice(q_base, q_base + q_rows)
        low = low_lanes((q_rows, LANES))
        query_low, query_high = query_block(x_ref, q_here, low)
        grad_low = grad_block(x_ref, q_here, low)
        peak = peak_ref[:, q_here]
        share = share_ref[:, q_here]
        term = jnp.zeros((8, q_rows), jnp.float32)
        for u_base, u_rows in blocks[: index + 1]:
            u_here = slice(u_base, u_base + u_rows)
            scores = score_tile(kq_ref, pc_ref, query_low, q_base, u_base, u_rows)
            soft = jnp.exp(scores - peak) * share
            s_ref[u_here, :q_rows] = soft
            soft_grad = dot_nt(x_ref[u_here, LANES:], grad_low)
            d_ref[u_here, :q_rows] = soft_grad
            term = term + folded(soft * soft_grad, jnp.sum)
        term = jnp.sum(term, axis=0, keepdims=True)
        query_grad = jnp.zeros((HEAD_DIM, q_rows), jnp.float32)
        for u_base, u_rows in blocks[: index + 1]:
            u_here = slice(u_base, u_base + u_rows)
            score_low = (s_ref[u_here, :q_rows] * (d_ref[u_here, :q_rows] - term)).astype(
                jnp.bfloat16
            )
            acc_ref[u_here] += dot_nn(score_low, query_high)
            query_grad = query_grad + dot_nn(kt_ref[:, u_here], score_low)
        query_grad = jnp.concatenate([query_grad, jnp.zeros_like(query_grad)], axis=0)
        acc_ref[q_here] += query_grad.T
    for base, rows in blocks:
        here = slice(base, base + rows)
        qk_ref[here] = (acc_ref[here] * scale).astype(jnp.bfloat16)


def unpack_value_kernel(place_ref, x_ref, mine_ref, away_ref):
    heads, kept, _ = x_ref.shape
    columns, tokens, _ = mine_ref.shape
    rest = tokens - kept
    cores = HEAD_DIM * columns // LANES
    quarter = HEAD_DIM // cores
    lane = lax.broadcasted_iota(jnp.int32, (tokens, LANES), 1)
    first_core = place_ref[0] == 0
    for column in range(columns):
        step = (column + columns - place_ref[1]) % columns
        parts = [jnp.zeros((tokens, LANES), jnp.float32)] * cores
        for group in range(heads // columns):
            block = x_ref[group * columns + column].astype(jnp.float32)
            for core in range(cores):
                home = group * quarter
                top = pltpu.roll(block, (home - core * quarter) % LANES, 1)
                bottom = pltpu.roll(block, (home - core * quarter - HEAD_DIM) % LANES, 1)[:rest]
                moved = jnp.concatenate([top, bottom], axis=0)
                inside = (lane >= home) & (lane < home + quarter)
                parts[core] = jnp.where(inside, moved, parts[core])
        mine_ref[step] = jnp.where(first_core, parts[0], parts[1]).astype(jnp.bfloat16)
        away_ref[step] = jnp.where(first_core, parts[1], parts[0]).astype(jnp.bfloat16)


def weight_open_kernel(x_ref, out_ref):
    for plane in range(x_ref.shape[0]):
        out_ref[:, plane * LANES : (plane + 1) * LANES] = x_ref[plane]


def weight_line_kernel(place_ref, *refs):
    pieces, out_ref = refs[:-1], refs[-1]
    lines = out_ref.shape[0]
    for step, piece_ref in enumerate(pieces):
        out_ref[(place_ref[1] + lines - step) % lines] = piece_ref[...]


def stack_kernel(*refs):
    for step, piece_ref in enumerate(refs[:-1]):
        refs[-1][step] = piece_ref[...]


def dot_tn(a, b):
    return lax.dot_general(a, b, (((0,), (0,)), ((), ())), preferred_element_type=jnp.float32)


def product_kernel(place_ref, own_ref, other_ref, *refs):
    columns = own_ref.shape[0]
    pieces, (block_ref,) = refs[:columns], refs[-1:]
    outs = refs[columns:-1]
    lines, w_cols, model = block_ref.shape
    width = 4 * LANES
    own = jnp.concatenate([piece[0] for piece in pieces], axis=0)
    other = jnp.concatenate([piece[1] for piece in pieces], axis=0)
    rows = own.shape[0]
    for base in range(0, model, width):
        cols = slice(base, base + width)
        total = dot_tn(own, own_ref[:, :, cols].reshape(rows, width))
        total = total + dot_tn(other, other_ref[:, :, cols].reshape(rows, width))
        block_ref[:, :, cols] = total.astype(jnp.bfloat16).reshape(lines, w_cols, width)
    for step, out_ref in enumerate(outs):
        out_ref[...] = block_ref[(place_ref[2] + step) % lines]


def input_grad_kernel(place_ref, first_ref, second_ref, *refs):
    columns, tokens, _ = first_ref.shape
    weight_ref = refs[-1]
    mine_ref, away_ref = refs[-3:-1]
    lines, w_cols = weight_ref.shape[1:3]
    for step, piece_ref in enumerate(refs[:-3]):
        for column in range(columns):
            weight_ref[column, (place_ref[2] + lines - step) % lines] = piece_ref[
                column * w_cols : (column + 1) * w_cols
            ]
    width = 4 * LANES
    for base in range(0, mine_ref.shape[1], width):
        cols = slice(base, base + width)
        first = jnp.zeros((tokens, width), jnp.float32)
        second = jnp.zeros((tokens, width), jnp.float32)
        for step in range(columns):
            weight = weight_ref[(place_ref[1] + step) % columns, :, :, cols]
            weight = weight.reshape(LANES, width)
            first = first + dot_nn(first_ref[step], weight)
            second = second + dot_nn(second_ref[step], weight)
        mine_ref[:, cols] = first
        away_ref[:, cols] = second.astype(jnp.bfloat16)


def add_kernel(first_ref, second_ref, out_ref):
    total = first_ref[...] + second_ref[...].astype(jnp.float32)
    out_ref[...] = total.astype(jnp.bfloat16)


def unpack_pair_kernel(x_ref, q_ref, k_ref):
    heads, tokens, _ = x_ref.shape
    low = low_lanes((tokens, LANES))
    for pair in range(heads // 2):
        first = x_ref[2 * pair].astype(jnp.float32)
        second = x_ref[2 * pair + 1].astype(jnp.float32)
        cols = slice(pair * LANES, (pair + 1) * LANES)
        q_ref[:, cols] = jnp.where(low, first, rolled(second)).astype(jnp.bfloat16)
        k_ref[:, cols] = jnp.where(low, rolled(first), second).astype(jnp.bfloat16)


def exchanged(x, axis):
    return lax.all_to_all(x, axis, split_axis=0, concat_axis=0, tiled=True)


def shifted(x, axis, step):
    count = lax.axis_size(axis)
    return lax.ppermute(x, axis, [(place, (place + step) % count) for place in range(count)])


def numbered(blocks, axis):
    sent = []
    for step in range(1, lax.axis_size(axis)):
        sent.append(shifted(blocks[step], axis, step))
    return sent


def from_all(x, axis):
    return [x] + [shifted(x, axis, step) for step in range(1, lax.axis_size(axis))]


def near(x):
    return pltpu.with_memory_space_constraint(x, pltpu.VMEM)


def shaped(*shape, dtype=jnp.bfloat16):
    return jax.ShapeDtypeStruct(shape, dtype)


def shards(inputs, query_vectors, key_vectors, value_vectors, cotangent, gate_prefix, value_weight):
    planes = lax.axis_size("sp")
    columns, lines = lax.axis_size("x"), lax.axis_size("y")
    core = lax.axis_index("core")
    tokens, model = inputs.shape[1:]
    width = query_vectors.shape[2]
    heads = width // HEAD_DIM
    length = planes * tokens
    w_cols = value_weight.shape[1]
    weight_block = jnp.broadcast_to(value_weight.T, (planes, w_cols, model // planes))
    weight_block = exchanged(weight_block, "sp")
    place = jnp.stack([core, lax.axis_index("x"), lax.axis_index("y")]).astype(jnp.int32)
    small, whole = pl.BlockSpec(memory_space=pltpu.SMEM), pl.BlockSpec(memory_space=pltpu.VMEM)
    weight_block = pl.pallas_call(weight_open_kernel, out_shape=shaped(w_cols, model))(
        near(weight_block)
    )
    packed = pl.pallas_call(pack_kernel, out_shape=shaped(heads, tokens, 2 * LANES))(
        query_vectors[0], key_vectors[0], value_vectors[0], cotangent[0]
    )
    arrived = exchanged(packed, "sp")
    own_rows = pl.pallas_call(stack_kernel, out_shape=shaped(columns, tokens, model))(
        inputs[0], *map(near, from_all(inputs[0], "x")[1:])
    )
    other_rows = shifted(own_rows, "core", 1)
    weight_line = pl.pallas_call(
        weight_line_kernel,
        out_shape=shaped(columns, w_cols, model),
        in_specs=[small] + [whole] * columns,
    )(place, weight_block, *map(near, from_all(weight_block, "x")[1:]))
    weight_line = weight_line.reshape(columns * w_cols, model)
    weight_pieces = from_all(weight_line, "y")
    kept = (tokens // 2 + 7) // 8 * 8
    sequence = near(arrived.reshape(length, 2 * LANES))
    wide, tile = pltpu.VMEM((length, LANES), jnp.float32), pltpu.VMEM((length, TILE), jnp.float32)
    row = shaped(1, length, dtype=jnp.float32)
    value_grad, peak, share = pl.pallas_call(
        value_kernel,
        out_shape=(shaped(planes, kept, LANES), row, row),
        scratch_shapes=[pltpu.VMEM((length, LANES), jnp.bfloat16), wide, wide, tile],
    )(sequence, gate_prefix[0])
    value_back = exchanged(value_grad, "sp")
    pair_grad = pl.pallas_call(
        pair_kernel,
        out_shape=shaped(length, LANES),
        scratch_shapes=[
            pltpu.VMEM((length, LANES), jnp.bfloat16),
            pltpu.VMEM((HEAD_DIM, length), jnp.bfloat16),
            wide,
            wide,
            tile,
            tile,
        ],
    )(sequence, gate_prefix[0], peak, share)
    pair_back = exchanged(pair_grad.reshape(planes, tokens, LANES), "sp")
    block = shaped(columns, tokens, LANES)
    mine, away = pl.pallas_call(
        unpack_value_kernel, out_shape=(block, block), in_specs=[small, whole]
    )(place, near(value_back))
    brought = shifted(away, "core", 1)
    both = jnp.stack([mine, brought], axis=1)
    pieces = [both[0]] + numbered(both, "x")
    partial = pl.pallas_call(
        product_kernel,
        compiler_params=pltpu.CompilerParams(vmem_limit_bytes=VMEM_BYTES),
        out_shape=(shaped(w_cols, model),) * lines,
        in_specs=[small] + [whole] * (2 + columns),
        scratch_shapes=[pltpu.VMEM((lines, w_cols, model), jnp.bfloat16)],
    )(place, near(own_rows), near(other_rows), *map(near, pieces))
    partial = [partial[0]] + numbered(partial, "y")
    partial = sum(part.astype(jnp.float32) for part in partial).astype(jnp.bfloat16)
    partial = jnp.moveaxis(partial.reshape(w_cols, planes, model // planes), 1, 0)
    partial = exchanged(partial, "sp")
    weight_grad = partial.astype(jnp.float32).sum(axis=0).T
    query_grad, key_grad = pl.pallas_call(
        unpack_pair_kernel, out_shape=(shaped(tokens, width), shaped(tokens, width))
    )(near(pair_back))
    kept_part, sent_part = pl.pallas_call(
        input_grad_kernel,
        out_shape=(shaped(tokens, model, dtype=jnp.float32), shaped(tokens, model)),
        in_specs=[small] + [whole] * (2 + lines),
        scratch_shapes=[pltpu.VMEM((columns, lines, w_cols, model), jnp.bfloat16)],
    )(place, mine, near(brought), *weight_pieces)
    input_grad = pl.pallas_call(add_kernel, out_shape=shaped(tokens, model))(
        kept_part, near(shifted(sent_part, "core", 1))
    )
    return (query_grad[None], key_grad[None], input_grad[None], weight_grad)


def solution(mesh):
    grid = Mesh(mesh.devices.reshape(-1, 4, 4, 2), ("sp", "y", "x", "core"))
    rows = P(("y", "x", "core"), "sp", None)
    weight = P("sp", ("y", "x", "core"))

    return jax.shard_map(
        shards,
        mesh=grid,
        in_specs=(rows,) * 6 + (weight,),
        out_specs=(rows, rows, rows, weight),
        check_vma=False,
    )
```
